512 devices in a mesh: kv: 128 (over z, x, core), tp: 4 (over y).
Axes of the slice: x: 4, y: 4, z: 16, core: 2. Of those that a mesh axis runs over, the one named last changes fastest.
Arguments:
- queries: bfloat16 [1024, 4, 8, 128], P('kv', None, 'tp'), may hold values from -6 to 6
- keys: bfloat16 [1024, 4, 8, 128], P('kv', None, 'tp'), may hold values from -6 to 6
- values: bfloat16 [1024, 4, 8, 256], P('kv', None, 'tp'), may hold values from -6 to 6
- in_gate: float32 [1024, 4, 8], P('kv', None, 'tp'), may hold values from -6 to 6
- forget_pre: float32 [1024, 4, 8], P('kv', None, 'tp'), may hold values from -1 to 5
- old_keys: bfloat16 [1024, 4, 8, 128], P('kv', None, 'tp'), may hold values from -6 to 6
- old_values: bfloat16 [1024, 4, 8, 256], P('kv', None, 'tp'), may hold values from -6 to 6
- old_in_gate: float32 [1024, 4, 8], P('kv', None, 'tp'), may hold values from -6 to 6
- old_forget: float32 [1024, 4, 8], P('kv', None, 'tp'), may hold values from -1 to 5
- accepted: int32 [1024], P('kv'), may hold values from 0 to 4
- state_mem: float32 [1024, 8, 128, 256], P('kv', 'tp'), may hold values from -4 to 4
- state_norm: float32 [1024, 8, 128], P('kv', 'tp'), may hold values from -6 to 6
- state_max: float32 [1024, 8], P('kv', 'tp'), may hold values from -4 to 4
- norm_gain: float32 [8, 256], P('tp'), may hold values from 0.1 to 1.9
- out_weight: bfloat16 [2048, 2048], P('tp', 'kv'), may hold values from -0.125 to 0.125
Outputs:
- mixed: bfloat16 [1024, 4, 2048], P('kv', 'tp')
- new_mem: float32 [1024, 8, 128, 256], P('kv', 'tp')
- new_norm: float32 [1024, 8, 128], P('kv', 'tp')
- new_max: float32 [1024, 8], P('kv', 'tp')
The draws below stay inside these ranges and needn't reach their ends.
Inputs may be any that keep to these rules, and one draw needn't show every extreme that they name: How many of the last step's 4 proposals of a sequence were accepted.
All inputs are finite; a program needn't handle non-finite values.
Results may differ from the reference program's by a relative error of at most 0.0068.
Values may be sent and summed in bfloat16 or wider, within the bound.
No kernel may reach another device: no remote copies, remote signals or barrier semaphores. Data moves between devices by JAX's collectives and lax.ppermute only.
A program may use at most 64 MiB of HBM per device.

```python
import jax
import jax.numpy as jnp
from jax import lax

D = 2048
HEADS = 8
DK = 128
DV = 256
PROPOSALS = 4
SEQS = 1024
HV = 2048


def with_ends(array, stream_key, least, largest):
    place = [jax.random.randint(jax.random.fold_in(stream_key, axis), (), 0, length) for axis, length in enumerate(array.shape)]
    main_axis = array.shape.index(max(array.shape))
    neighbour = place[:main_axis] + [(place[main_axis] + 1) % array.shape[main_axis]] + place[main_axis + 1:]
    return array.at[tuple(place)].set(least).at[tuple(neighbour)].set(largest)


def levels(own_key, dims, shards, smallest, high):
    gain, own = 1.0, jax.random.fold_in(own_key, 6)
    for axis_at, shards_of in shards:
        steps = jnp.exp(jax.random.uniform(jax.random.fold_in(own, axis_at), (shards_of,), jnp.float32, smallest / len(shards), high / len(shards)))
        gain = gain * jnp.repeat(steps, dims[axis_at] // shards_of).reshape([-1 if axis == axis_at else 1 for axis in range(len(dims))])
    return gain


def normal_values(rng, dims, deviation, reach, pieces=(), kind=jnp.bfloat16):
    gain = levels(rng, dims, pieces, -0.22, 0.18) if pieces else 1.0
    values = jax.random.normal(rng, dims, jnp.float32) * deviation * gain
    return jnp.minimum(jnp.maximum(values, -reach), reach).astype(kind)


def setup_inputs(seed: int = 0) -> dict:
    streams_of = jax.random.split(jax.random.key(seed), 16)
    queries = normal_values(streams_of[0], (SEQS, PROPOSALS, HEADS, DK), 1.0, 6.0, ((0, 128), (2, 4)))
    keys = normal_values(streams_of[1], (SEQS, PROPOSALS, HEADS, DK), 1.0, 6.0, ((0, 128), (2, 4)))
    values = normal_values(streams_of[2], (SEQS, PROPOSALS, HEADS, DV), 1.0, 6.0, ((0, 128), (2, 4)))
    in_gate = normal_values(streams_of[3], (SEQS, PROPOSALS, HEADS), 1.0, 6.0, ((0, 128), (2, 4)), jnp.float32)
    forget_pre = jnp.clip(-1.0 + 6.0 * jax.random.uniform(streams_of[4], (SEQS, PROPOSALS, HEADS), jnp.float32) ** levels(streams_of[4], (SEQS, PROPOSALS, HEADS), ((0, 128), (2, 4)), -0.2, 0.2), -1.0, 5.0)
    old_keys = normal_values(streams_of[5], (SEQS, PROPOSALS, HEADS, DK), 1.0, 6.0, ((0, 128), (2, 4)))
    old_values = normal_values(streams_of[6], (SEQS, PROPOSALS, HEADS, DV), 1.0, 6.0, ((0, 128), (2, 4)))
    old_in_gate = normal_values(streams_of[7], (SEQS, PROPOSALS, HEADS), 1.0, 6.0, ((0, 128), (2, 4)), jnp.float32)
    old_forget = jnp.clip(-1.0 + 6.0 * jax.random.uniform(streams_of[8], (SEQS, PROPOSALS, HEADS), jnp.float32) ** levels(streams_of[8], (SEQS, PROPOSALS, HEADS), ((0, 128), (2, 4)), -0.2, 0.2), -1.0, 5.0)
    accepted = with_ends(jax.random.randint(streams_of[9], (SEQS,), 0, PROPOSALS + 1), jax.random.fold_in(streams_of[9], 1), 0, PROPOSALS).astype(jnp.int32)
    state_mem = normal_values(streams_of[10], (SEQS, HEADS, DK, DV), 0.3, 4.0, ((0, 128), (1, 4)), jnp.float32)
    state_norm = normal_values(streams_of[11], (SEQS, HEADS, DK), 0.5, 6.0, ((0, 128), (1, 4)), jnp.float32)
    state_max = normal_values(streams_of[12], (SEQS, HEADS), 1.0, 4.0, ((0, 128), (1, 4)), jnp.float32)
    norm_gain = jnp.clip(1.0 + 0.18 * jax.random.normal(streams_of[13], (HEADS, DV), jnp.float32), 0.1, 1.9)
    out_weight = normal_values(streams_of[14], (HV, D), HV ** -0.5, 0.125, ((0, 4), (1, 128)))
    return dict(queries=queries, keys=keys, values=values, in_gate=in_gate, forget_pre=forget_pre, old_keys=old_keys, old_values=old_values, old_in_gate=old_in_gate, old_forget=old_forget, accepted=accepted, state_mem=state_mem, state_norm=state_norm, state_max=state_max, norm_gain=norm_gain, out_weight=out_weight)


HIGH = lax.Precision.HIGHEST

def cell(queries, keys, values, in_gates, log_forget, memory, normal, stab):
    length = in_gates.shape[-1]
    causal = jnp.tril(jnp.ones((length, length), dtype=bool))
    cumul = jnp.cumsum(log_forget, axis=-1)
    logd = jnp.where(causal, cumul[:, :, None] - cumul[:, None, :] + in_gates[:, None, :], -jnp.inf)
    inter = cumul + stab[:, None]
    m_row = jnp.maximum(inter, lax.optimization_barrier(jnp.max(logd, axis=-1)))
    scores = jnp.einsum('hld,hsd->hls', queries, keys, precision=HIGH) * jnp.exp(logd - m_row[..., None])
    w_inter = jnp.exp(inter - m_row)
    num = w_inter[..., None] * jnp.einsum('hld,hde->hle', queries, memory, precision=HIGH) + jnp.einsum('hls,hse->hle', scores, values, precision=HIGH)
    den = w_inter * jnp.einsum('hld,hd->hl', queries, normal, precision=HIGH) + lax.optimization_barrier(jnp.sum(scores, axis=-1))
    hidden = num / jnp.maximum(jnp.abs(den), 1.0)[..., None]
    m_new = m_row[:, -1]
    g_state = jnp.exp(cumul[:, -1] + stab - m_new)
    g_tok = jnp.exp(cumul[:, -1:] - cumul + in_gates - m_new[:, None])
    mem_new = g_state[:, None, None] * memory + jnp.einsum('hld,hle->hde', g_tok[..., None] * keys, values, precision=HIGH)
    norm_new = g_state[:, None] * normal + jnp.einsum('hl,hld->hd', g_tok, keys, precision=HIGH)
    return (hidden, mem_new, norm_new, m_new)

def one_sequence(items):
    queries, keys, values, in_gate, forget_pre, old_keys, old_values, old_in_gate, old_forget, accepted, memory, normal, stab, norm_gain = items
    props = queries.shape[0]
    live = jnp.arange(props, dtype=jnp.int32) < accepted
    gates = jnp.concatenate([jnp.where(live[:, None], old_in_gate, -jnp.inf), in_gate], axis=0)
    forget = jnp.concatenate([jnp.where(live[:, None], jax.nn.log_sigmoid(old_forget), 0.0), jax.nn.log_sigmoid(forget_pre)], axis=0)
    scale = queries.shape[-1] ** (-0.5)
    qrun = jnp.concatenate([jnp.zeros(queries.shape, jnp.float32), queries.astype(jnp.float32) * scale], axis=0)
    krun = jnp.concatenate([old_keys, keys], axis=0).astype(jnp.float32)
    vrun = jnp.concatenate([old_values, values], axis=0).astype(jnp.float32)
    hidden, mem_new, norm_new, m_new = cell(jnp.swapaxes(qrun, 0, 1), jnp.swapaxes(krun, 0, 1), jnp.swapaxes(vrun, 0, 1), gates.T, forget.T, memory, normal, stab)
    hidden = hidden[:, props:, :]
    mean = lax.optimization_barrier(jnp.mean(hidden, -1, keepdims=True))
    var = lax.optimization_barrier(jnp.mean(jnp.square(hidden - mean), -1, keepdims=True))
    normed = (hidden - mean) * lax.rsqrt(var + 1e-05) * norm_gain[:, None, :]
    flat = jnp.swapaxes(normed, 0, 1).reshape(props, -1).astype(jnp.bfloat16)
    return (flat, mem_new, norm_new, m_new)

def reference(queries, keys, values, in_gate, forget_pre, old_keys, old_values, old_in_gate, old_forget, accepted, state_mem, state_norm, state_max, norm_gain, out_weight):

    def apply(items):
        return one_sequence(items + (norm_gain,))
    hidden, new_mem, new_norm, new_max = lax.map(apply, (queries, keys, values, in_gate, forget_pre, old_keys, old_values, old_in_gate, old_forget, accepted, state_mem, state_norm, state_max))
    seqs, props, width = hidden.shape
    flat = hidden.reshape(seqs * props, width)
    total = jnp.dot(flat, out_weight, preferred_element_type=jnp.float32)
    mixed = total.astype(jnp.bfloat16).reshape(seqs, props, -1)
    return (mixed, new_mem, new_norm, new_max)
```

```python
import jax
import jax.numpy as jnp
from jax import lax
from jax.experimental import pallas as pl
from jax.experimental.pallas import tpu as pltpu
from jax.sharding import Mesh
from jax.sharding import PartitionSpec as P

KV = ("kv_0", "kv_1", "kv_2")
PLANE = ("kv_1", "kv_2")

SEQS = 8
PROPS = 4
HEADS = 2
DK = 128
DV = 256
ROWS = SEQS * PROPS * HEADS
RUN = 2 * ROWS
ITEMS = SEQS * HEADS
CHUNK = 4
CHUNKS = ITEMS // CHUNK
EPS = 1e-5


def iota(shape, dim):
    return lax.broadcasted_iota(jnp.int32, shape, dim)


def item_of(row):
    return (row // 8) % 8 * 2 + row % 2


def place_of(row):
    return row // 64 * 4 + row // 2 % 4


def exact_dot(a, b):
    return jnp.dot(a, b, precision=lax.Precision.HIGHEST, preferred_element_type=jnp.float32)


def halves(x):
    high = x.astype(jnp.bfloat16)
    return high, (x - high.astype(jnp.float32)).astype(jnp.bfloat16)


def dot_bt(a, b):
    return lax.dot_general(a, b, (((1,), (1,)), ((), ())), preferred_element_type=jnp.float32)


def log_sigmoid(x):
    return jnp.minimum(x, 0.0) - jnp.log1p(jnp.exp(-jnp.abs(x)))


def state_copies(state_hbm, state, sems):
    return [
        pltpu.make_async_copy(
            state_hbm.at[pl.ds(c * CHUNK, CHUNK)], state.at[pl.ds(c * CHUNK, CHUNK)], sems.at[c]
        )
        for c in range(CHUNKS)
    ]


def hidden_kernel(
    q_ref, k_ref, ko_ref, v_ref, vo_ref, ig_ref, fg_ref, igo_ref, fgo_ref, acc_ref, smax_ref,
    norm_ref, gain_ref, state_hbm, hidden_ref, coef_ref, state, flat, sems,
):
    copies = state_copies(state_hbm, state, sems)
    for copy in copies:
        copy.start()

    lane1 = iota((1, RUN), 1)
    parts = []
    for ref in (igo_ref, ig_ref, fgo_ref, fg_ref):
        parts.append(jnp.concatenate([ref[p] for p in range(PROPS)], axis=0))
    parts.append(
        jnp.concatenate(
            [smax_ref[...], acc_ref[...].astype(jnp.float32), jnp.zeros((5, SEQS), jnp.float32)],
            axis=0,
        )
    )
    spread = (iota((SEQS, RUN), 1) % 64 // 8 == iota((SEQS, RUN), 0)).astype(jnp.float32)
    wide = exact_dot(jnp.concatenate(parts, axis=0), spread)
    own = iota((8, RUN), 0) == iota((8, RUN), 1) % 8
    rows = [
        jnp.sum(jnp.where(own, wide[8 * a : 8 * a + 8], 0.0), axis=0, keepdims=True)
        for a in range(4)
    ]
    smax = jnp.where(lane1 % 2 == 0, wide[32:33], wide[33:34])
    old = lane1 < ROWS
    live = (lane1 // 2 % 4).astype(jnp.float32) < wide[34:35]
    ig = jnp.where(old, jnp.where(live, rows[0], -jnp.inf), rows[1])
    forget = log_sigmoid(jnp.where(old, rows[2], rows[3]))
    forget = jnp.where(old & ~live, 0.0, forget)

    src, dst = iota((RUN, RUN), 0), iota((RUN, RUN), 1)
    together = item_of(src) == item_of(dst)
    upto = (together & (place_of(src) <= place_of(dst))).astype(jnp.float32)
    sums = exact_dot(
        jnp.broadcast_to(forget, (8, RUN)),
        jnp.concatenate([upto, together.astype(jnp.float32)], axis=1),
    )
    b = sums[0:1, :RUN]
    b_last = sums[0:1, RUN:]

    qrow, lane = iota((ROWS, RUN), 0), iota((ROWS, RUN), 1)
    same = item_of(qrow) == item_of(lane)
    valid = same & (place_of(lane) <= PROPS + qrow // 2 % 4)
    at = lane == ROWS + qrow
    b_col = jnp.sum(jnp.where(at, b, 0.0), axis=1, keepdims=True)
    inter = jnp.sum(jnp.where(at, b + smax, 0.0), axis=1, keepdims=True)
    logd = jnp.where(valid, b_col + (ig - b), -jnp.inf)
    m_row = jnp.maximum(inter, jnp.max(logd, axis=1, keepdims=True))
    decay = jnp.exp(logd - m_row)
    w_inter = jnp.exp(inter - m_row)

    last = same & (qrow // 2 % 4 == PROPS - 1)
    new_max = jnp.sum(jnp.where(last, m_row, 0.0), axis=0, keepdims=True)
    coef_ref[0:1, :] = jnp.exp(b_last - b + ig - new_max)
    coef_ref[1:2, :] = jnp.exp(b_last + smax - new_max)
    coef_ref[2:3, :] = new_max
    coef_ref[3:8, :] = jnp.zeros((5, RUN), jnp.float32)

    scale = DK**-0.5
    q = q_ref[...]
    k = jnp.concatenate([ko_ref[...], k_ref[...]], axis=0)
    v = jnp.concatenate([vo_ref[...], v_ref[...]], axis=0)
    probs = dot_bt(q, k) * scale * decay
    p_high, p_low = halves(probs)
    intra = jnp.dot(p_high, v, preferred_element_type=jnp.float32) + jnp.dot(
        p_low, v, preferred_element_type=jnp.float32
    )
    qn = lax.dot_general(
        q.astype(jnp.float32), norm_ref[...], (((1,), (1,)), ((), ())),
        precision=lax.Precision.HIGHEST, preferred_element_type=jnp.float32,
    )
    mine = item_of(iota((ROWS, ITEMS), 0)) == iota((ROWS, ITEMS), 1)
    qn = jnp.sum(jnp.where(mine, qn, 0.0), axis=1, keepdims=True)
    w_scaled = w_inter * scale
    den = w_scaled * qn + jnp.sum(probs, axis=1, keepdims=True)
    inv = 1.0 / jnp.maximum(jnp.abs(den), 1.0)
    gain = jnp.where(iota((ROWS // CHUNKS, DV), 0) % 2 == 0, gain_ref[0:1, :], gain_ref[1:2, :])

    size = ROWS // CHUNKS
    for c in range(CHUNKS):
        lo, hi = c * size, (c + 1) * size
        qc = q[lo:hi].astype(jnp.float32)
        item = item_of(iota((size, DK), 0) + lo)
        lhs = jnp.concatenate(
            [jnp.where(item == c * CHUNK + i, qc, 0.0) for i in range(CHUNK)], axis=1
        ).astype(jnp.bfloat16)
        copies[c].wait()
        s_high, s_low = halves(state[pl.ds(c * CHUNK, CHUNK)].reshape(CHUNK * DK, DV))
        num = jnp.dot(lhs, s_high, preferred_element_type=jnp.float32) + jnp.dot(
            lhs, s_low, preferred_element_type=jnp.float32
        )
        h = (w_scaled[lo:hi] * num + intra[lo:hi]) * inv[lo:hi]
        h = h - jnp.mean(h, axis=1, keepdims=True)
        var = jnp.mean(h * h, axis=1, keepdims=True)
        h = h * lax.rsqrt(var + EPS) * gain
        for half in range(2):
            flat[half, lo:hi, :] = h[:, half * DK : (half + 1) * DK]
    for p in range(PROPS):
        for head in range(HEADS):
            for half in range(2):
                piece = flat[half, pl.ds(p * HEADS + head, SEQS, stride=8), :]
                at = head * DV + half * DK
                hidden_ref[p, :, at : at + DK] = piece.astype(jnp.bfloat16)


def memory_kernel(
    coef_ref, k_ref, ko_ref, v_ref, vo_ref, norm_ref, state_hbm,
    new_hbm, new_norm_ref, state, new, sems, out_sems,
):
    copies = state_copies(state_hbm, state, sems)
    for copy in copies:
        copy.start()
    tok, keep = coef_ref[0:1, :], coef_ref[1:2, :]
    k = jnp.concatenate([ko_ref[...], k_ref[...]], axis=0).astype(jnp.float32)
    v = jnp.concatenate([vo_ref[...], v_ref[...]], axis=0)
    lane = iota((ITEMS, RUN), 1)
    mine = item_of(lane) == iota((ITEMS, RUN), 0)
    t_high, t_low = halves(jnp.where(mine, tok, 0.0))
    kb = k.astype(jnp.bfloat16)
    kept = jnp.sum(jnp.where(mine & (place_of(lane) == 0), keep, 0.0), axis=1, keepdims=True)
    new_norm_ref[...] = (
        kept * norm_ref[...]
        + jnp.dot(t_high, kb, preferred_element_type=jnp.float32)
        + jnp.dot(t_low, kb, preferred_element_type=jnp.float32)
    )
    weighted = k.T * tok
    twice = jnp.concatenate([v, v], axis=0)
    lane = item_of(iota((DK, RUN), 1))
    stores = []
    for c in range(CHUNKS):
        copies[c].wait()
        for i in range(c * CHUNK, (c + 1) * CHUNK):
            high, low = halves(jnp.where(lane == i, weighted, 0.0))
            update = jnp.dot(
                jnp.concatenate([high, low], axis=1), twice, preferred_element_type=jnp.float32
            )
            at = i // 2 * 8 + i % 2
            new[i] = keep[:, at : at + 1] * state[i] + update
        stores.append(
            pltpu.make_async_copy(
                new.at[pl.ds(c * CHUNK, CHUNK)], new_hbm.at[pl.ds(c * CHUNK, CHUNK)], out_sems.at[c]
            )
        )
        stores[-1].start()
    for store in stores:
        store.wait()


VMEM = pl.BlockSpec(memory_space=pltpu.VMEM)
ANY = pl.BlockSpec(memory_space=pl.ANY)


def hidden_of(q, k, ko, v, vo, ig, fg, igo, fgo, accepted, smax, norm, gain, state):
    return pl.pallas_call(
        hidden_kernel,
        in_specs=[VMEM] * 13 + [ANY],
        out_specs=(VMEM, VMEM),
        out_shape=(
            jax.ShapeDtypeStruct((PROPS, SEQS, HEADS * DV), jnp.bfloat16),
            jax.ShapeDtypeStruct((8, RUN), jnp.float32),
        ),
        scratch_shapes=[
            pltpu.VMEM((ITEMS, DK, DV), jnp.float32),
            pltpu.VMEM((2, ROWS, DK), jnp.float32),
            pltpu.SemaphoreType.DMA((CHUNKS,)),
        ],
        name="hidden",
    )(q, k, ko, v, vo, ig, fg, igo, fgo, accepted, smax, norm, gain, state)


def memory_of(coef, k, ko, v, vo, norm, state):
    return pl.pallas_call(
        memory_kernel,
        in_specs=[VMEM] * 6 + [ANY],
        out_specs=(ANY, VMEM),
        out_shape=(
            jax.ShapeDtypeStruct((ITEMS, DK, DV), jnp.float32),
            jax.ShapeDtypeStruct((ITEMS, DK), jnp.float32),
        ),
        scratch_shapes=[
            pltpu.VMEM((ITEMS, DK, DV), jnp.float32),
            pltpu.VMEM((ITEMS, DK, DV), jnp.float32),
            pltpu.SemaphoreType.DMA((CHUNKS,)),
            pltpu.SemaphoreType.DMA((CHUNKS,)),
        ],
        name="memory",
    )(coef, k, ko, v, vo, norm, state)


def to_each(block, count):
    return jnp.broadcast_to(block[None], (count, *block.shape))


def exchanged(pieces, axes):
    return lax.all_to_all(pieces, axes, split_axis=0, concat_axis=0, tiled=True)


def on_device(
    queries,
    keys,
    values,
    in_gate,
    forget_pre,
    old_keys,
    old_values,
    old_in_gate,
    old_forget,
    accepted,
    state_mem,
    state_norm,
    state_max,
    norm_gain,
    out_weight,
):
    zs, cross, tps = lax.axis_size("kv_0"), lax.axis_size(PLANE), lax.axis_size("tp")
    weight = exchanged(to_each(out_weight.T, zs), "kv_0")
    weight = weight.reshape(-1, out_weight.shape[0])
    q, k, ko, v, vo = (
        a.reshape(ROWS, -1) for a in (queries, keys, old_keys, values, old_values)
    )
    gates = (
        a.transpose(1, 2, 0) for a in (in_gate, forget_pre, old_in_gate, old_forget)
    )
    norm = state_norm.reshape(ITEMS, DK)
    state = state_mem.reshape(ITEMS, DK, DV)
    hidden, coef = hidden_of(
        q, k, ko, v, vo, *gates, accepted[None], state_max.T, norm, norm_gain, state
    )
    rows = lax.all_gather(hidden.reshape(PROPS * SEQS, -1), PLANE, tiled=True)
    new_mem, new_norm = memory_of(coef, k, ko, v, vo, norm, state)
    terms = lax.dot_general(
        rows, weight, (((1,), (1,)), ((), ())), preferred_element_type=jnp.float32
    ).astype(jnp.bfloat16)
    terms = exchanged(terms.reshape(cross * tps, SEQS, -1), (*PLANE, "tp"))
    total = terms.astype(jnp.float32).reshape(cross, tps, SEQS, zs, -1).sum(axis=1)
    mixed = total.astype(jnp.bfloat16).transpose(1, 2, 0, 3).reshape(SEQS, 1, -1)
    new_max = coef[2, :ROWS].reshape(SEQS, PROPS, HEADS)[:, 0]
    return (
        mixed,
        new_mem.reshape(state_mem.shape),
        new_norm.reshape(state_norm.shape),
        new_max,
    )


def solution(mesh):
    finer = Mesh(mesh.devices.reshape(16, 4, 2, mesh.shape["tp"]), (*KV, "tp"))
    in_specs = (
        P(KV, None, "tp", None),
        P(KV, None, "tp", None),
        P(KV, None, "tp", None),
        P(KV, None, "tp"),
        P(KV, None, "tp"),
        P(KV, None, "tp", None),
        P(KV, None, "tp", None),
        P(KV, None, "tp"),
        P(KV, None, "tp"),
        P(KV),
        P(KV, "tp", None, None),
        P(KV, "tp", None),
        P(KV, "tp"),
        P("tp", None),
        P("tp", KV),
    )
    out_specs = (P(KV, "tp", None), P(KV, "tp", None, None), P(KV, "tp", None), P(KV, "tp"))
    return jax.shard_map(
        on_device, mesh=finer, in_specs=in_specs, out_specs=out_specs, check_vma=False
    )
```

```python
import functools

import jax
import jax.numpy as jnp
from jax import lax
from jax.experimental import pallas as pl
from jax.experimental.pallas import tpu as pltpu
from jax.sharding import Mesh
from jax.sharding import PartitionSpec as P

KV = ("kv_0", "kv_1", "kv_2")
PLANE = ("kv_1", "kv_2")

SEQS = 8
PROPS = 4
HEADS = 2
DK = 128
DV = 256
ROWS = SEQS * PROPS * HEADS
RUN = 2 * ROWS
ITEMS = SEQS * HEADS
CHUNK = 4
CHUNKS = ITEMS // CHUNK
EPS = 1e-5


def iota(shape, dim):
    return lax.broadcasted_iota(jnp.int32, shape, dim)


def item_of(row):
    return (row // 8) % 8 * 2 + row % 2


def place_of(row):
    return row // 64 * 4 + row // 2 % 4


def exact_dot(a, b):
    return jnp.dot(a, b, precision=lax.Precision.HIGHEST, preferred_element_type=jnp.float32)


def halves(x):
    high = x.astype(jnp.bfloat16)
    return high, (x - high.astype(jnp.float32)).astype(jnp.bfloat16)


def dot_bt(a, b):
    return lax.dot_general(a, b, (((1,), (1,)), ((), ())), preferred_element_type=jnp.float32)


def log_sigmoid(x):
    return jnp.minimum(x, 0.0) - jnp.log1p(jnp.exp(-jnp.abs(x)))


def in_row_order(view):
    dst, src = iota((RUN, RUN), 0), iota((RUN, RUN), 1)
    row = dst % ROWS
    pick = src == row // 2 * 4 + dst // ROWS * 2 + row % 2
    rows = jnp.dot(pick.astype(jnp.bfloat16), view, preferred_element_type=jnp.float32)
    return jnp.concatenate([rows[:ROWS], rows[ROWS:]], axis=1).astype(jnp.bfloat16)


def state_copies(state_hbm, state, sems):
    return [
        pltpu.make_async_copy(
            state_hbm.at[pl.ds(c * CHUNK, CHUNK)], state.at[pl.ds(c * CHUNK, CHUNK)], sems.at[c]
        )
        for c in range(CHUNKS)
    ]


def hidden_kernel(
    q_ref, k_ref, ko_ref, v_ref, vo_ref, ig_ref, fg_ref, igo_ref, fgo_ref, acc_ref, smax_ref,
    norm_ref, gain_ref, state_hbm, hidden_ref, coef_ref, values_ref, state, flat, sems,
):
    copies = state_copies(state_hbm, state, sems)
    for copy in copies:
        copy.start()

    lane1 = iota((1, RUN), 1)
    parts = []
    for ref in (igo_ref, ig_ref, fgo_ref, fg_ref):
        parts.append(jnp.concatenate([ref[p] for p in range(PROPS)], axis=0))
    parts.append(
        jnp.concatenate(
            [smax_ref[...], acc_ref[...].astype(jnp.float32), jnp.zeros((5, SEQS), jnp.float32)],
            axis=0,
        )
    )
    spread = (iota((SEQS, RUN), 1) % 64 // 8 == iota((SEQS, RUN), 0)).astype(jnp.float32)
    wide = exact_dot(jnp.concatenate(parts, axis=0), spread)
    own = iota((8, RUN), 0) == iota((8, RUN), 1) % 8
    rows = [
        jnp.sum(jnp.where(own, wide[8 * a : 8 * a + 8], 0.0), axis=0, keepdims=True)
        for a in range(4)
    ]
    smax = jnp.where(lane1 % 2 == 0, wide[32:33], wide[33:34])
    old = lane1 < ROWS
    live = (lane1 // 2 % 4).astype(jnp.float32) < wide[34:35]
    ig = jnp.where(old, jnp.where(live, rows[0], -jnp.inf), rows[1])
    forget = log_sigmoid(jnp.where(old, rows[2], rows[3]))
    forget = jnp.where(old & ~live, 0.0, forget)

    src, dst = iota((RUN, RUN), 0), iota((RUN, RUN), 1)
    together = item_of(src) == item_of(dst)
    upto = (together & (place_of(src) <= place_of(dst))).astype(jnp.float32)
    sums = exact_dot(
        jnp.broadcast_to(forget, (8, RUN)),
        jnp.concatenate([upto, together.astype(jnp.float32)], axis=1),
    )
    b = sums[0:1, :RUN]
    b_last = sums[0:1, RUN:]

    qrow, lane = iota((ROWS, RUN), 0), iota((ROWS, RUN), 1)
    same = item_of(qrow) == item_of(lane)
    valid = same & (place_of(lane) <= PROPS + qrow // 2 % 4)
    at = lane == ROWS + qrow
    b_col = jnp.sum(jnp.where(at, b, 0.0), axis=1, keepdims=True)
    inter = jnp.sum(jnp.where(at, b + smax, 0.0), axis=1, keepdims=True)
    logd = jnp.where(valid, b_col + (ig - b), -jnp.inf)
    m_row = jnp.maximum(inter, jnp.max(logd, axis=1, keepdims=True))
    decay = jnp.exp(logd - m_row)
    w_inter = jnp.exp(inter - m_row)

    last = same & (qrow // 2 % 4 == PROPS - 1)
    new_max = jnp.sum(jnp.where(last, m_row, 0.0), axis=0, keepdims=True)
    coef_ref[0:1, :] = jnp.exp(b_last - b + ig - new_max)
    coef_ref[1:2, :] = jnp.exp(b_last + smax - new_max)
    coef_ref[2:3, :] = new_max
    coef_ref[3:8, :] = jnp.zeros((5, RUN), jnp.float32)

    scale = DK**-0.5
    q = q_ref[...]
    k = jnp.concatenate([ko_ref[...], k_ref[...]], axis=0)
    v = jnp.concatenate([in_row_order(vo_ref[...]), in_row_order(v_ref[...])], axis=0)
    values_ref[...] = v
    probs = dot_bt(q, k) * scale * decay
    p_high, p_low = halves(probs)
    intra = jnp.dot(p_high, v, preferred_element_type=jnp.float32) + jnp.dot(
        p_low, v, preferred_element_type=jnp.float32
    )
    qn = lax.dot_general(
        q.astype(jnp.float32), norm_ref[...], (((1,), (1,)), ((), ())),
        precision=lax.Precision.HIGHEST, preferred_element_type=jnp.float32,
    )
    mine = item_of(iota((ROWS, ITEMS), 0)) == iota((ROWS, ITEMS), 1)
    qn = jnp.sum(jnp.where(mine, qn, 0.0), axis=1, keepdims=True)
    w_scaled = w_inter * scale
    den = w_scaled * qn + jnp.sum(probs, axis=1, keepdims=True)
    inv = 1.0 / jnp.maximum(jnp.abs(den), 1.0)
    gain = jnp.where(iota((ROWS // CHUNKS, DV), 0) % 2 == 0, gain_ref[0:1, :], gain_ref[1:2, :])

    size = ROWS // CHUNKS
    for c in range(CHUNKS):
        lo, hi = c * size, (c + 1) * size
        qc = q[lo:hi].astype(jnp.float32)
        item = item_of(iota((size, DK), 0) + lo)
        lhs = jnp.concatenate(
            [jnp.where(item == c * CHUNK + i, qc, 0.0) for i in range(CHUNK)], axis=1
        ).astype(jnp.bfloat16)
        copies[c].wait()
        s_high, s_low = halves(state[pl.ds(c * CHUNK, CHUNK)].reshape(CHUNK * DK, DV))
        num = jnp.dot(lhs, s_high, preferred_element_type=jnp.float32) + jnp.dot(
            lhs, s_low, preferred_element_type=jnp.float32
        )
        h = (w_scaled[lo:hi] * num + intra[lo:hi]) * inv[lo:hi]
        h = h - jnp.mean(h, axis=1, keepdims=True)
        var = jnp.mean(h * h, axis=1, keepdims=True)
        h = h * lax.rsqrt(var + EPS) * gain
        for half in range(2):
            flat[half, lo:hi, :] = h[:, half * DK : (half + 1) * DK]
    for p in range(PROPS):
        for head in range(HEADS):
            for half in range(2):
                piece = flat[half, pl.ds(p * HEADS + head, SEQS, stride=8), :]
                at = head * DV + half * DK
                hidden_ref[p, :, at : at + DK] = piece.astype(jnp.bfloat16)


def memory_kernel(
    coef_ref, k_ref, ko_ref, values_ref, norm_ref, state_hbm,
    new_hbm, new_norm_ref, new_max_ref, state, new, sems, out_sems,
):
    copies = state_copies(state_hbm, state, sems)
    for copy in copies:
        copy.start()
    tok, keep = coef_ref[0:1, :], coef_ref[1:2, :]
    k = jnp.concatenate([ko_ref[...], k_ref[...]], axis=0).astype(jnp.float32)
    v = values_ref[...]
    lane = iota((8, RUN), 1)
    first = (place_of(lane) == 0) & (lane % 2 == iota((8, RUN), 0))
    seq = (iota((RUN, SEQS), 0) // 8 % 8 == iota((RUN, SEQS), 1)).astype(jnp.float32)
    new_max_ref[...] = exact_dot(jnp.where(first, coef_ref[2:3, :], 0.0), seq)[:HEADS]
    lane = iota((ITEMS, RUN), 1)
    mine = item_of(lane) == iota((ITEMS, RUN), 0)
    t_high, t_low = halves(jnp.where(mine, tok, 0.0))
    kb = k.astype(jnp.bfloat16)
    kept = jnp.sum(jnp.where(mine & (place_of(lane) == 0), keep, 0.0), axis=1, keepdims=True)
    new_norm_ref[...] = (
        kept * norm_ref[...]
        + jnp.dot(t_high, kb, preferred_element_type=jnp.float32)
        + jnp.dot(t_low, kb, preferred_element_type=jnp.float32)
    )
    weighted = k.T * tok
    twice = jnp.concatenate([v, v], axis=0)
    lane = item_of(iota((DK, RUN), 1))
    stores = []
    for c in range(CHUNKS):
        copies[c].wait()
        for i in range(c * CHUNK, (c + 1) * CHUNK):
            high, low = halves(jnp.where(lane == i, weighted, 0.0))
            update = jnp.dot(
                jnp.concatenate([high, low], axis=1), twice, preferred_element_type=jnp.float32
            )
            at = i // 2 * 8 + i % 2
            new[i] = keep[:, at : at + 1] * state[i] + update
        stores.append(
            pltpu.make_async_copy(
                new.at[pl.ds(c * CHUNK, CHUNK)], new_hbm.at[pl.ds(c * CHUNK, CHUNK)], out_sems.at[c]
            )
        )
        stores[-1].start()
    for store in stores:
        store.wait()


VMEM = pl.BlockSpec(memory_space=pltpu.VMEM)
ANY = pl.BlockSpec(memory_space=pl.ANY)


def hidden_of(q, k, ko, v, vo, ig, fg, igo, fgo, accepted, smax, norm, gain, state):
    return pl.pallas_call(
        hidden_kernel,
        in_specs=[VMEM] * 13 + [ANY],
        out_specs=(VMEM, VMEM, VMEM),
        out_shape=(
            pltpu.VMEM((PROPS, SEQS, HEADS * DV), jnp.bfloat16),
            pltpu.VMEM((8, RUN), jnp.float32),
            pltpu.VMEM((RUN, DV), jnp.bfloat16),
        ),
        scratch_shapes=[
            pltpu.VMEM((ITEMS, DK, DV), jnp.float32),
            pltpu.VMEM((2, ROWS, DK), jnp.float32),
            pltpu.SemaphoreType.DMA((CHUNKS,)),
        ],
        name="hidden",
    )(q, k, ko, v, vo, ig, fg, igo, fgo, accepted, smax, norm, gain, state)


def memory_of(coef, k, ko, v, norm, state):
    return pl.pallas_call(
        memory_kernel,
        in_specs=[VMEM] * 5 + [ANY],
        out_specs=(ANY, VMEM, VMEM),
        out_shape=(
            jax.ShapeDtypeStruct((ITEMS, DK, DV), jnp.float32),
            jax.ShapeDtypeStruct((ITEMS, DK), jnp.float32),
            jax.ShapeDtypeStruct((HEADS, SEQS), jnp.float32),
        ),
        scratch_shapes=[
            pltpu.VMEM((ITEMS, DK, DV), jnp.float32),
            pltpu.VMEM((ITEMS, DK, DV), jnp.float32),
            pltpu.SemaphoreType.DMA((CHUNKS,)),
            pltpu.SemaphoreType.DMA((CHUNKS,)),
        ],
        name="memory",
    )(coef, k, ko, v, norm, state)


def copies_kernel(block_ref, out_ref):
    for i in range(out_ref.shape[0]):
        out_ref[i] = block_ref[...]


def to_each(block, count):
    return pl.pallas_call(
        copies_kernel,
        in_specs=[VMEM],
        out_specs=VMEM,
        out_shape=pltpu.VMEM((count, *block.shape), block.dtype),
        name="to_each",
    )(block)


def join_kernel(terms_ref, out_ref, *, tps, block):
    cross = terms_ref.shape[0] // tps
    lane = iota((SEQS, DK), 1) // block
    for part in range(terms_ref.shape[2] // DK):
        cols = slice(part * DK, (part + 1) * DK)
        sums = [
            sum(terms_ref[g * tps + t, :, cols].astype(jnp.float32) for t in range(tps))
            for g in range(cross)
        ]
        step = 1
        while step < cross:
            low = lane & step == 0
            swapped = list(sums)
            for g in range(cross):
                if g & step == 0:
                    a, b = sums[g], sums[g + step]
                    swapped[g] = jnp.where(low, a, pltpu.roll(b, step * block, 1))
                    swapped[g + step] = jnp.where(low, pltpu.roll(a, DK - step * block, 1), b)
            sums = swapped
            step *= 2
        for z in range(cross):
            at = (part * cross + z) * DK
            out_ref[:, at : at + DK] = sums[z].astype(jnp.bfloat16)


def joined(terms, tps, block):
    sources, seqs, cols = terms.shape
    return pl.pallas_call(
        functools.partial(join_kernel, tps=tps, block=block),
        in_specs=[VMEM],
        out_specs=VMEM,
        out_shape=jax.ShapeDtypeStruct((seqs, sources // tps * cols), jnp.bfloat16),
        name="join",
    )(terms)


def exchanged(pieces, axes):
    return lax.all_to_all(pieces, axes, split_axis=0, concat_axis=0, tiled=True)


def on_device(
    queries,
    keys,
    values,
    in_gate,
    forget_pre,
    old_keys,
    old_values,
    old_in_gate,
    old_forget,
    accepted,
    state_mem,
    state_norm,
    state_max,
    norm_gain,
    out_weight,
):
    zs, cross, tps = lax.axis_size("kv_0"), lax.axis_size(PLANE), lax.axis_size("tp")
    weight = exchanged(to_each(out_weight.T, zs), "kv_0")
    weight = weight.reshape(-1, out_weight.shape[0])
    q, k, ko = (a.reshape(ROWS, DK) for a in (queries, keys, old_keys))
    v, vo = (
        a.reshape(SEQS, PROPS, HEADS, 2, DK).swapaxes(2, 3).reshape(RUN, DK)
        for a in (values, old_values)
    )
    gates = (
        a.transpose(1, 2, 0) for a in (in_gate, forget_pre, old_in_gate, old_forget)
    )
    norm = state_norm.reshape(ITEMS, DK)
    state = state_mem.reshape(ITEMS, DK, DV)
    hidden, coef, run_values = hidden_of(
        q, k, ko, v, vo, *gates, accepted[None], state_max.T, norm, norm_gain, state
    )
    rows = lax.all_gather(hidden.reshape(PROPS * SEQS, -1), PLANE, tiled=True)
    terms = lax.dot_general(
        rows, weight, (((1,), (1,)), ((), ())), preferred_element_type=jnp.float32
    ).astype(jnp.bfloat16)
    terms = exchanged(terms.reshape(cross * tps, SEQS, -1), (*PLANE, "tp"))
    coef, run_values = (
        pltpu.with_memory_space_constraint(a, pltpu.VMEM) for a in (coef, run_values)
    )
    new_mem, new_norm, new_max = memory_of(coef, k, ko, run_values, norm, state)
    terms = pltpu.with_memory_space_constraint(terms, pltpu.VMEM)
    mixed = joined(terms, tps, out_weight.shape[1])[:, None]
    return (
        mixed,
        new_mem.reshape(state_mem.shape),
        new_norm.reshape(state_norm.shape),
        new_max.T,
    )


def solution(mesh):
    finer = Mesh(mesh.devices.reshape(16, 4, 2, mesh.shape["tp"]), (*KV, "tp"))
    in_specs = (
        P(KV, None, "tp", None),
        P(KV, None, "tp", None),
        P(KV, None, "tp", None),
        P(KV, None, "tp"),
        P(KV, None, "tp"),
        P(KV, None, "tp", None),
        P(KV, None, "tp", None),
        P(KV, None, "tp"),
        P(KV, None, "tp"),
        P(KV),
        P(KV, "tp", None, None),
        P(KV, "tp", None),
        P(KV, "tp"),
        P("tp", None),
        P("tp", KV),
    )
    out_specs = (P(KV, "tp", None), P(KV, "tp", None, None), P(KV, "tp", None), P(KV, "tp"))
    return jax.shard_map(
        on_device, mesh=finer, in_specs=in_specs, out_specs=out_specs, check_vma=False
    )
```

```python
import functools

import jax
import jax.numpy as jnp
from jax import lax
from jax.experimental import pallas as pl
from jax.experimental.pallas import tpu as pltpu
from jax.sharding import Mesh
from jax.sharding import PartitionSpec as P

KV = ("kv_0", "kv_1", "kv_2")

SEQS = 8
PROPS = 4
HEADS = 2
DK = 128
DV = 256
ROWS = SEQS * PROPS * HEADS
RUN = 2 * ROWS
ITEMS = SEQS * HEADS
CHUNK = 4
CHUNKS = ITEMS // CHUNK
EPS = 1e-5


def iota(shape, dim):
    return lax.broadcasted_iota(jnp.int32, shape, dim)


def item_of(row):
    return (row // 8) % 8 * 2 + row % 2


def place_of(row):
    return row // 64 * 4 + row // 2 % 4


def exact_dot(a, b):
    return jnp.dot(a, b, precision=lax.Precision.HIGHEST, preferred_element_type=jnp.float32)


def halves(x):
    high = x.astype(jnp.bfloat16)
    return high, (x - high.astype(jnp.float32)).astype(jnp.bfloat16)


def dot_bt(a, b):
    return lax.dot_general(a, b, (((1,), (1,)), ((), ())), preferred_element_type=jnp.float32)


def log_sigmoid(x):
    return jnp.minimum(x, 0.0) - jnp.log1p(jnp.exp(-jnp.abs(x)))


def in_row_order(view):
    dst, src = iota((RUN, RUN), 0), iota((RUN, RUN), 1)
    row = dst % ROWS
    pick = src == row // 2 * 4 + dst // ROWS * 2 + row % 2
    rows = jnp.dot(pick.astype(jnp.bfloat16), view, preferred_element_type=jnp.float32)
    return jnp.concatenate([rows[:ROWS], rows[ROWS:]], axis=1).astype(jnp.bfloat16)


def state_copies(state_hbm, state, sems):
    return [
        pltpu.make_async_copy(
            state_hbm.at[pl.ds(c * CHUNK, CHUNK)], state.at[pl.ds(c * CHUNK, CHUNK)], sems.at[c]
        )
        for c in range(CHUNKS)
    ]


def hidden_kernel(
    q_ref, k_ref, ko_ref, v_ref, vo_ref, ig_ref, fg_ref, igo_ref, fgo_ref, acc_ref, smax_ref,
    norm_ref, gain_ref, state_hbm, hidden_ref, coef_ref, values_ref, state, flat, sems,
):
    copies = state_copies(state_hbm, state, sems)
    for copy in copies:
        copy.start()

    lane1 = iota((1, RUN), 1)
    parts = []
    for ref in (igo_ref, ig_ref, fgo_ref, fg_ref):
        parts.append(jnp.concatenate([ref[p] for p in range(PROPS)], axis=0))
    parts.append(
        jnp.concatenate(
            [smax_ref[...], acc_ref[...].astype(jnp.float32), jnp.zeros((5, SEQS), jnp.float32)],
            axis=0,
        )
    )
    spread = (iota((SEQS, RUN), 1) % 64 // 8 == iota((SEQS, RUN), 0)).astype(jnp.float32)
    wide = exact_dot(jnp.concatenate(parts, axis=0), spread)
    own = iota((8, RUN), 0) == iota((8, RUN), 1) % 8
    rows = [
        jnp.sum(jnp.where(own, wide[8 * a : 8 * a + 8], 0.0), axis=0, keepdims=True)
        for a in range(4)
    ]
    smax = jnp.where(lane1 % 2 == 0, wide[32:33], wide[33:34])
    old = lane1 < ROWS
    live = (lane1 // 2 % 4).astype(jnp.float32) < wide[34:35]
    ig = jnp.where(old, jnp.where(live, rows[0], -jnp.inf), rows[1])
    forget = log_sigmoid(jnp.where(old, rows[2], rows[3]))
    forget = jnp.where(old & ~live, 0.0, forget)

    src, dst = iota((RUN, RUN), 0), iota((RUN, RUN), 1)
    together = item_of(src) == item_of(dst)
    upto = (together & (place_of(src) <= place_of(dst))).astype(jnp.float32)
    sums = exact_dot(
        jnp.broadcast_to(forget, (8, RUN)),
        jnp.concatenate([upto, together.astype(jnp.float32)], axis=1),
    )
    b = sums[0:1, :RUN]
    b_last = sums[0:1, RUN:]

    qrow, lane = iota((ROWS, RUN), 0), iota((ROWS, RUN), 1)
    same = item_of(qrow) == item_of(lane)
    valid = same & (place_of(lane) <= PROPS + qrow // 2 % 4)
    at = lane == ROWS + qrow
    b_col = jnp.sum(jnp.where(at, b, 0.0), axis=1, keepdims=True)
    inter = jnp.sum(jnp.where(at, b + smax, 0.0), axis=1, keepdims=True)
    logd = jnp.where(valid, b_col + (ig - b), -jnp.inf)
    m_row = jnp.maximum(inter, jnp.max(logd, axis=1, keepdims=True))
    decay = jnp.exp(logd - m_row)
    w_inter = jnp.exp(inter - m_row)

    last = same & (qrow // 2 % 4 == PROPS - 1)
    new_max = jnp.sum(jnp.where(last, m_row, 0.0), axis=0, keepdims=True)
    coef_ref[0:1, :] = jnp.exp(b_last - b + ig - new_max)
    coef_ref[1:2, :] = jnp.exp(b_last + smax - new_max)
    coef_ref[2:3, :] = new_max
    coef_ref[3:8, :] = jnp.zeros((5, RUN), jnp.float32)

    scale = DK**-0.5
    q = q_ref[...]
    k = jnp.concatenate([ko_ref[...], k_ref[...]], axis=0)
    v = jnp.concatenate([in_row_order(vo_ref[...]), in_row_order(v_ref[...])], axis=0)
    values_ref[...] = v
    probs = dot_bt(q, k) * scale * decay
    p_high, p_low = halves(probs)
    intra = jnp.dot(p_high, v, preferred_element_type=jnp.float32) + jnp.dot(
        p_low, v, preferred_element_type=jnp.float32
    )
    qn = lax.dot_general(
        q.astype(jnp.float32), norm_ref[...], (((1,), (1,)), ((), ())),
        precision=lax.Precision.HIGHEST, preferred_element_type=jnp.float32,
    )
    mine = item_of(iota((ROWS, ITEMS), 0)) == iota((ROWS, ITEMS), 1)
    qn = jnp.sum(jnp.where(mine, qn, 0.0), axis=1, keepdims=True)
    w_scaled = w_inter * scale
    den = w_scaled * qn + jnp.sum(probs, axis=1, keepdims=True)
    inv = 1.0 / jnp.maximum(jnp.abs(den), 1.0)
    gain = jnp.where(iota((ROWS // CHUNKS, DV), 0) % 2 == 0, gain_ref[0:1, :], gain_ref[1:2, :])

    for copy in copies:
        copy.wait()
    size = ROWS // CHUNKS
    for c in range(CHUNKS):
        lo, hi = c * size, (c + 1) * size
        qc = q[lo:hi].astype(jnp.float32)
        item = item_of(iota((size, DK), 0) + lo)
        lhs = jnp.concatenate(
            [jnp.where(item == c * CHUNK + i, qc, 0.0) for i in range(CHUNK)], axis=1
        ).astype(jnp.bfloat16)
        s_high, s_low = halves(state[pl.ds(c * CHUNK, CHUNK)].reshape(CHUNK * DK, DV))
        num = jnp.dot(lhs, s_high, preferred_element_type=jnp.float32) + jnp.dot(
            lhs, s_low, preferred_element_type=jnp.float32
        )
        h = (w_scaled[lo:hi] * num + intra[lo:hi]) * inv[lo:hi]
        h = h - jnp.mean(h, axis=1, keepdims=True)
        var = jnp.mean(h * h, axis=1, keepdims=True)
        h = h * lax.rsqrt(var + EPS) * gain
        for half in range(2):
            flat[half, lo:hi, :] = h[:, half * DK : (half + 1) * DK]
    for p in range(PROPS):
        for head in range(HEADS):
            for half in range(2):
                piece = flat[half, pl.ds(p * HEADS + head, SEQS, stride=8), :]
                at = head * DV + half * DK
                hidden_ref[p, :, at : at + DK] = piece.astype(jnp.bfloat16)


def memory_kernel(
    coef_ref, k_ref, ko_ref, values_ref, norm_ref, state_hbm,
    new_hbm, new_norm_ref, new_max_ref, state, new, sems, out_sems,
):
    copies = state_copies(state_hbm, state, sems)
    for copy in copies:
        copy.start()
    tok, keep = coef_ref[0:1, :], coef_ref[1:2, :]
    k = jnp.concatenate([ko_ref[...], k_ref[...]], axis=0).astype(jnp.float32)
    v = values_ref[...]
    lane = iota((8, RUN), 1)
    first = (place_of(lane) == 0) & (lane % 2 == iota((8, RUN), 0))
    seq = (iota((RUN, SEQS), 0) // 8 % 8 == iota((RUN, SEQS), 1)).astype(jnp.float32)
    new_max_ref[...] = exact_dot(jnp.where(first, coef_ref[2:3, :], 0.0), seq)[:HEADS]
    lane = iota((ITEMS, RUN), 1)
    mine = item_of(lane) == iota((ITEMS, RUN), 0)
    t_high, t_low = halves(jnp.where(mine, tok, 0.0))
    kb = k.astype(jnp.bfloat16)
    kept = jnp.sum(jnp.where(mine & (place_of(lane) == 0), keep, 0.0), axis=1, keepdims=True)
    new_norm_ref[...] = (
        kept * norm_ref[...]
        + jnp.dot(t_high, kb, preferred_element_type=jnp.float32)
        + jnp.dot(t_low, kb, preferred_element_type=jnp.float32)
    )
    weighted = k.T * tok
    twice = jnp.concatenate([v, v], axis=0)
    lane = item_of(iota((DK, RUN), 1))
    stores = []
    for c in range(CHUNKS):
        copies[c].wait()
        for i in range(c * CHUNK, (c + 1) * CHUNK):
            high, low = halves(jnp.where(lane == i, weighted, 0.0))
            update = jnp.dot(
                jnp.concatenate([high, low], axis=1), twice, preferred_element_type=jnp.float32
            )
            at = i // 2 * 8 + i % 2
            new[i] = keep[:, at : at + 1] * state[i] + update
        stores.append(
            pltpu.make_async_copy(
                new.at[pl.ds(c * CHUNK, CHUNK)], new_hbm.at[pl.ds(c * CHUNK, CHUNK)], out_sems.at[c]
            )
        )
        stores[-1].start()
    for store in stores:
        store.wait()


VMEM = pl.BlockSpec(memory_space=pltpu.VMEM)
SMEM = pl.BlockSpec(memory_space=pltpu.SMEM)
ANY = pl.BlockSpec(memory_space=pl.ANY)


def hidden_of(q, k, ko, v, vo, ig, fg, igo, fgo, accepted, smax, norm, gain, state):
    return pl.pallas_call(
        hidden_kernel,
        in_specs=[VMEM] * 13 + [ANY],
        out_specs=(VMEM, VMEM, VMEM),
        out_shape=(
            pltpu.VMEM((PROPS, SEQS, HEADS * DV), jnp.bfloat16),
            pltpu.VMEM((8, RUN), jnp.float32),
            pltpu.VMEM((RUN, DV), jnp.bfloat16),
        ),
        scratch_shapes=[
            pltpu.VMEM((ITEMS, DK, DV), jnp.float32),
            pltpu.VMEM((2, ROWS, DK), jnp.float32),
            pltpu.SemaphoreType.DMA((CHUNKS,)),
        ],
        name="hidden",
    )(q, k, ko, v, vo, ig, fg, igo, fgo, accepted, smax, norm, gain, state)


def memory_of(coef, k, ko, v, norm, state):
    return pl.pallas_call(
        memory_kernel,
        in_specs=[VMEM] * 5 + [ANY],
        out_specs=(ANY, VMEM, VMEM),
        out_shape=(
            jax.ShapeDtypeStruct((ITEMS, DK, DV), jnp.float32),
            jax.ShapeDtypeStruct((ITEMS, DK), jnp.float32),
            jax.ShapeDtypeStruct((HEADS, SEQS), jnp.float32),
        ),
        scratch_shapes=[
            pltpu.VMEM((ITEMS, DK, DV), jnp.float32),
            pltpu.VMEM((ITEMS, DK, DV), jnp.float32),
            pltpu.SemaphoreType.DMA((CHUNKS,)),
            pltpu.SemaphoreType.DMA((CHUNKS,)),
        ],
        name="memory",
    )(coef, k, ko, v, norm, state)


def copies_kernel(block_ref, out_ref):
    for i in range(out_ref.shape[0]):
        out_ref[i] = block_ref[...]


def to_each(block, count):
    return pl.pallas_call(
        copies_kernel,
        in_specs=[VMEM],
        out_specs=VMEM,
        out_shape=pltpu.VMEM((count, *block.shape), block.dtype),
        name="to_each",
    )(block)


def product_kernel(x_ref, *refs):
    *row_refs, own_ref, swapped_ref, out_ref = refs
    rows = jnp.concatenate([ref[...] for ref in row_refs], axis=0)
    size = own_ref.shape[0]
    for half, ref in enumerate((own_ref, swapped_ref)):
        terms = dot_bt(rows, ref[...]).astype(jnp.bfloat16)
        for d in range(len(row_refs)):
            for p in range(PROPS):
                at = (d * PROPS + p) * SEQS
                out_ref[(x_ref[0] ^ d) * PROPS + p, :, half * size : (half + 1) * size] = terms[
                    at : at + SEQS
                ]


def product(x, rows, own, swapped):
    return pl.pallas_call(
        product_kernel,
        in_specs=[SMEM] + [VMEM] * (len(rows) + 2),
        out_specs=VMEM,
        out_shape=jax.ShapeDtypeStruct(
            (len(rows) * PROPS, SEQS, 2 * own.shape[0]), jnp.bfloat16
        ),
        name="product",
    )(x, *rows, own, swapped)


def join_kernel(core_ref, terms_ref, out_ref, *, tps, block):
    cross, size = terms_ref.shape[0] // tps * 2, terms_ref.shape[2] // 2
    lane = iota((SEQS, DK), 1) // block
    swap = jnp.full((SEQS, DK), core_ref[0], jnp.int32) == 1
    for part in range(size // DK):
        sums = []
        for g in range(cross // 2):
            pair = []
            for half in range(2):
                at = half * size + part * DK
                pair.append(
                    sum(
                        terms_ref[g * tps + t, :, at : at + DK].astype(jnp.float32)
                        for t in range(tps)
                    )
                )
            own, other = pair
            sums += [jnp.where(swap, other, own), jnp.where(swap, own, other)]
        step = 1
        while step < cross:
            low = lane & step == 0
            swapped = list(sums)
            for g in range(cross):
                if g & step == 0:
                    a, b = sums[g], sums[g + step]
                    swapped[g] = jnp.where(low, a, pltpu.roll(b, step * block, 1))
                    swapped[g + step] = jnp.where(low, pltpu.roll(a, DK - step * block, 1), b)
            sums = swapped
            step *= 2
        for z in range(cross):
            at = (part * cross + z) * DK
            out_ref[:, at : at + DK] = sums[z].astype(jnp.bfloat16)


def joined(core, terms, tps, block):
    sources, seqs, cols = terms.shape
    return pl.pallas_call(
        functools.partial(join_kernel, tps=tps, block=block),
        in_specs=[SMEM, VMEM],
        out_specs=VMEM,
        out_shape=jax.ShapeDtypeStruct((seqs, sources // tps * cols), jnp.bfloat16),
        name="join",
    )(core, terms)


def in_vmem(array):
    return pltpu.with_memory_space_constraint(array, pltpu.VMEM)


def exchanged(pieces, axes):
    return lax.all_to_all(pieces, axes, split_axis=0, concat_axis=0, tiled=True)


def traded(block, axis, d):
    return lax.ppermute(block, axis, [(i, i ^ d) for i in range(lax.axis_size(axis))])


def on_device(
    queries,
    keys,
    values,
    in_gate,
    forget_pre,
    old_keys,
    old_values,
    old_in_gate,
    old_forget,
    accepted,
    state_mem,
    state_norm,
    state_max,
    norm_gain,
    out_weight,
):
    zs, xs, tps = lax.axis_size("kv_0"), lax.axis_size("kv_1"), lax.axis_size("tp")
    own = exchanged(to_each(out_weight.T, zs), "kv_0")
    own = own.reshape(-1, out_weight.shape[0])
    q, k, ko = (a.reshape(ROWS, DK) for a in (queries, keys, old_keys))
    v, vo = (
        a.reshape(SEQS, PROPS, HEADS, 2, DK).swapaxes(2, 3).reshape(RUN, DK)
        for a in (values, old_values)
    )
    gates = (
        a.transpose(1, 2, 0) for a in (in_gate, forget_pre, old_in_gate, old_forget)
    )
    norm = state_norm.reshape(ITEMS, DK)
    state = state_mem.reshape(ITEMS, DK, DV)
    hidden, coef, run_values = hidden_of(
        q, k, ko, v, vo, *gates, accepted[None], state_max.T, norm, norm_gain, state
    )
    hidden = hidden.reshape(PROPS * SEQS, -1)
    rows = [hidden]
    for d in range(1, xs):
        rows.append(traded(hidden, "kv_1", d))
    swapped = traded(own, "kv_2", 1)
    place = [lax.axis_index(a)[None].astype(jnp.int32) for a in ("kv_1", "kv_2")]
    *rows, own, swapped = (in_vmem(a) for a in (*rows, own, swapped))
    terms = product(place[0], rows, own, swapped)
    terms = exchanged(terms, ("kv_1", "tp"))
    new_mem, new_norm, new_max = memory_of(in_vmem(coef), k, ko, in_vmem(run_values), norm, state)
    mixed = joined(place[1], in_vmem(terms), tps, out_weight.shape[1])[:, None]
    return (
        mixed,
        new_mem.reshape(state_mem.shape),
        new_norm.reshape(state_norm.shape),
        new_max.T,
    )


def solution(mesh):
    finer = Mesh(mesh.devices.reshape(16, 4, 2, mesh.shape["tp"]), (*KV, "tp"))
    in_specs = (
        P(KV, None, "tp", None),
        P(KV, None, "tp", None),
        P(KV, None, "tp", None),
        P(KV, None, "tp"),
        P(KV, None, "tp"),
        P(KV, None, "tp", None),
        P(KV, None, "tp", None),
        P(KV, None, "tp"),
        P(KV, None, "tp"),
        P(KV),
        P(KV, "tp", None, None),
        P(KV, "tp", None),
        P(KV, "tp"),
        P("tp", None),
        P("tp", KV),
    )
    out_specs = (P(KV, "tp", None), P(KV, "tp", None, None), P(KV, "tp", None), P(KV, "tp"))
    return jax.shard_map(
        on_device, mesh=finer, in_specs=in_specs, out_specs=out_specs, check_vma=False
    )
```

```python
import functools

import jax
import jax.numpy as jnp
from jax import lax
from jax.experimental import pallas as pl
from jax.experimental.pallas import tpu as pltpu
from jax.sharding import Mesh
from jax.sharding import PartitionSpec as P

KV = ("kv_0", "kv_1", "kv_2")
PLANE = ("kv_1", "kv_2")

SEQS = 8
PROPS = 4
HEADS = 2
DK = 128
DV = 256
ROWS = SEQS * PROPS * HEADS
RUN = 2 * ROWS
ITEMS = SEQS * HEADS
CHUNK = 4
CHUNKS = ITEMS // CHUNK
KEPT = 8
EPS = 1e-5
FIRST_Z, FIRST_CROSS, FIRST_TP = 0, 5, 2


def iota(shape, dim):
    return lax.broadcasted_iota(jnp.int32, shape, dim)


def item_of(row):
    return (row // 8) % 8 * 2 + row % 2


def place_of(row):
    return row // 64 * 4 + row // 2 % 4


def exact_dot(a, b):
    return jnp.dot(a, b, precision=lax.Precision.HIGHEST, preferred_element_type=jnp.float32)


def halves(x):
    high = x.astype(jnp.bfloat16)
    return high, (x - high.astype(jnp.float32)).astype(jnp.bfloat16)


def dot_bt(a, b):
    return lax.dot_general(a, b, (((1,), (1,)), ((), ())), preferred_element_type=jnp.float32)


def log_sigmoid(x):
    return jnp.minimum(x, 0.0) - jnp.log1p(jnp.exp(-jnp.abs(x)))


def in_row_order(view):
    dst, src = iota((RUN, RUN), 0), iota((RUN, RUN), 1)
    row = dst % ROWS
    pick = src == row // 2 * 4 + dst // ROWS * 2 + row % 2
    rows = jnp.dot(pick.astype(jnp.bfloat16), view, preferred_element_type=jnp.float32)
    return jnp.concatenate([rows[:ROWS], rows[ROWS:]], axis=1).astype(jnp.bfloat16)


def state_copies(state_hbm, rest, sems):
    return [
        pltpu.make_async_copy(
            state_hbm.at[pl.ds(at, CHUNK)], rest.at[pl.ds(at - KEPT, CHUNK)], sems.at[i]
        )
        for i, at in enumerate(range(KEPT, ITEMS, CHUNK))
    ]


def hidden_kernel(
    q_ref, k_ref, ko_ref, v_ref, vo_ref, ig_ref, fg_ref, igo_ref, fgo_ref, acc_ref, smax_ref,
    norm_ref, gain_ref, kept, state_hbm, hidden_ref, coef_ref, values_ref, rest, flat, sems,
):
    copies = state_copies(state_hbm, rest, sems)
    for copy in copies:
        copy.start()

    lane1 = iota((1, RUN), 1)
    parts = []
    for ref in (igo_ref, ig_ref, fgo_ref, fg_ref):
        parts.append(jnp.concatenate([ref[p] for p in range(PROPS)], axis=0))
    parts.append(
        jnp.concatenate(
            [smax_ref[...], acc_ref[...].astype(jnp.float32), jnp.zeros((5, SEQS), jnp.float32)],
            axis=0,
        )
    )
    spread = (iota((SEQS, RUN), 1) % 64 // 8 == iota((SEQS, RUN), 0)).astype(jnp.float32)
    wide = exact_dot(jnp.concatenate(parts, axis=0), spread)
    own = iota((8, RUN), 0) == iota((8, RUN), 1) % 8
    rows = [
        jnp.sum(jnp.where(own, wide[8 * a : 8 * a + 8], 0.0), axis=0, keepdims=True)
        for a in range(4)
    ]
    smax = jnp.where(lane1 % 2 == 0, wide[32:33], wide[33:34])
    old = lane1 < ROWS
    live = (lane1 // 2 % 4).astype(jnp.float32) < wide[34:35]
    ig = jnp.where(old, jnp.where(live, rows[0], -jnp.inf), rows[1])
    forget = log_sigmoid(jnp.where(old, rows[2], rows[3]))
    forget = jnp.where(old & ~live, 0.0, forget)

    src, dst = iota((RUN, RUN), 0), iota((RUN, RUN), 1)
    together = item_of(src) == item_of(dst)
    upto = (together & (place_of(src) <= place_of(dst))).astype(jnp.float32)
    sums = exact_dot(
        jnp.broadcast_to(forget, (8, RUN)),
        jnp.concatenate([upto, together.astype(jnp.float32)], axis=1),
    )
    b = sums[0:1, :RUN]
    b_last = sums[0:1, RUN:]

    qrow, lane = iota((ROWS, RUN), 0), iota((ROWS, RUN), 1)
    same = item_of(qrow) == item_of(lane)
    valid = same & (place_of(lane) <= PROPS + qrow // 2 % 4)
    at = lane == ROWS + qrow
    b_col = jnp.sum(jnp.where(at, b, 0.0), axis=1, keepdims=True)
    inter = jnp.sum(jnp.where(at, b + smax, 0.0), axis=1, keepdims=True)
    logd = jnp.where(valid, b_col + (ig - b), -jnp.inf)
    m_row = jnp.maximum(inter, jnp.max(logd, axis=1, keepdims=True))
    decay = jnp.exp(logd - m_row)
    w_inter = jnp.exp(inter - m_row)

    last = same & (qrow // 2 % 4 == PROPS - 1)
    new_max = jnp.sum(jnp.where(last, m_row, 0.0), axis=0, keepdims=True)
    coef_ref[0:1, :] = jnp.exp(b_last - b + ig - new_max)
    coef_ref[1:2, :] = jnp.exp(b_last + smax - new_max)
    coef_ref[2:3, :] = new_max
    coef_ref[3:8, :] = jnp.zeros((5, RUN), jnp.float32)

    scale = DK**-0.5
    q = q_ref[...]
    k = jnp.concatenate([ko_ref[...], k_ref[...]], axis=0)
    v = jnp.concatenate([in_row_order(vo_ref[...]), in_row_order(v_ref[...])], axis=0)
    values_ref[...] = v
    probs = dot_bt(q, k) * scale * decay
    p_high, p_low = halves(probs)
    intra = jnp.dot(p_high, v, preferred_element_type=jnp.float32) + jnp.dot(
        p_low, v, preferred_element_type=jnp.float32
    )
    qn = lax.dot_general(
        q.astype(jnp.float32), norm_ref[...], (((1,), (1,)), ((), ())),
        precision=lax.Precision.HIGHEST, preferred_element_type=jnp.float32,
    )
    mine = item_of(iota((ROWS, ITEMS), 0)) == iota((ROWS, ITEMS), 1)
    qn = jnp.sum(jnp.where(mine, qn, 0.0), axis=1, keepdims=True)
    w_scaled = w_inter * scale
    den = w_scaled * qn + jnp.sum(probs, axis=1, keepdims=True)
    inv = 1.0 / jnp.maximum(jnp.abs(den), 1.0)
    gain = jnp.where(iota((ROWS // CHUNKS, DV), 0) % 2 == 0, gain_ref[0:1, :], gain_ref[1:2, :])

    for copy in copies:
        copy.wait()
    size = ROWS // CHUNKS
    for c in range(CHUNKS):
        lo, hi = c * size, (c + 1) * size
        qc = q[lo:hi].astype(jnp.float32)
        item = item_of(iota((size, DK), 0) + lo)
        lhs = jnp.concatenate(
            [jnp.where(item == c * CHUNK + i, qc, 0.0) for i in range(CHUNK)], axis=1
        ).astype(jnp.bfloat16)
        at = c * CHUNK
        part = kept[pl.ds(at, CHUNK)] if at < KEPT else rest[pl.ds(at - KEPT, CHUNK)]
        s_high, s_low = halves(part.reshape(CHUNK * DK, DV))
        num = jnp.dot(lhs, s_high, preferred_element_type=jnp.float32) + jnp.dot(
            lhs, s_low, preferred_element_type=jnp.float32
        )
        h = (w_scaled[lo:hi] * num + intra[lo:hi]) * inv[lo:hi]
        h = h - jnp.mean(h, axis=1, keepdims=True)
        var = jnp.mean(h * h, axis=1, keepdims=True)
        h = h * lax.rsqrt(var + EPS) * gain
        for half in range(2):
            flat[half, lo:hi, :] = h[:, half * DK : (half + 1) * DK]
    for p in range(PROPS):
        for head in range(HEADS):
            for half in range(2):
                piece = flat[half, pl.ds(p * HEADS + head, SEQS, stride=8), :]
                at = head * DV + half * DK
                hidden_ref[p, :, at : at + DK] = piece.astype(jnp.bfloat16)


def memory_kernel(
    coef_ref, k_ref, ko_ref, values_ref, norm_ref, kept, state_hbm,
    new_hbm, new_norm_ref, new_max_ref, rest, new, sems, out_sems,
):
    copies = state_copies(state_hbm, rest, sems)
    for copy in copies:
        copy.start()
    tok, keep = coef_ref[0:1, :], coef_ref[1:2, :]
    k = jnp.concatenate([ko_ref[...], k_ref[...]], axis=0).astype(jnp.float32)
    v = values_ref[...]
    lane = iota((8, RUN), 1)
    first = (place_of(lane) == 0) & (lane % 2 == iota((8, RUN), 0))
    seq = (iota((RUN, SEQS), 0) // 8 % 8 == iota((RUN, SEQS), 1)).astype(jnp.float32)
    new_max_ref[...] = exact_dot(jnp.where(first, coef_ref[2:3, :], 0.0), seq)[:HEADS]
    lane = iota((ITEMS, RUN), 1)
    mine = item_of(lane) == iota((ITEMS, RUN), 0)
    t_high, t_low = halves(jnp.where(mine, tok, 0.0))
    kb = k.astype(jnp.bfloat16)
    share = jnp.sum(jnp.where(mine & (place_of(lane) == 0), keep, 0.0), axis=1, keepdims=True)
    new_norm_ref[...] = (
        share * norm_ref[...]
        + jnp.dot(t_high, kb, preferred_element_type=jnp.float32)
        + jnp.dot(t_low, kb, preferred_element_type=jnp.float32)
    )
    high, low = halves(k.T * tok)
    both = jnp.concatenate([high, low], axis=1)
    twice = jnp.concatenate([v, v], axis=0)
    lane = item_of(iota((8, 2 * RUN), 1) % RUN)
    stores = []
    for c in range(CHUNKS):
        if c * CHUNK >= KEPT:
            copies[c - KEPT // CHUNK].wait()
        for i in range(c * CHUNK, (c + 1) * CHUNK):
            mask = (lane == i).astype(jnp.float32)[:1].astype(jnp.bfloat16)
            update = jnp.dot(both * mask, twice, preferred_element_type=jnp.float32)
            at = i // 2 * 8 + i % 2
            old = kept[i] if i < KEPT else rest[i - KEPT]
            new[i] = keep[:, at : at + 1] * old + update
        stores.append(
            pltpu.make_async_copy(
                new.at[pl.ds(c * CHUNK, CHUNK)], new_hbm.at[pl.ds(c * CHUNK, CHUNK)], out_sems.at[c]
            )
        )
        stores[-1].start()
    for store in stores:
        store.wait()


VMEM = pl.BlockSpec(memory_space=pltpu.VMEM)
ANY = pl.BlockSpec(memory_space=pl.ANY)


def hidden_of(q, k, ko, v, vo, ig, fg, igo, fgo, accepted, smax, norm, gain, kept, state):
    return pl.pallas_call(
        hidden_kernel,
        in_specs=[VMEM] * 14 + [ANY],
        out_specs=(VMEM, VMEM, VMEM),
        out_shape=(
            pltpu.VMEM((PROPS, SEQS, HEADS * DV), jnp.bfloat16),
            pltpu.VMEM((8, RUN), jnp.float32),
            pltpu.VMEM((RUN, DV), jnp.bfloat16),
        ),
        scratch_shapes=[
            pltpu.VMEM((ITEMS - KEPT, DK, DV), jnp.float32),
            pltpu.VMEM((2, ROWS, DK), jnp.float32),
            pltpu.SemaphoreType.DMA((CHUNKS,)),
        ],
        name="hidden",
    )(q, k, ko, v, vo, ig, fg, igo, fgo, accepted, smax, norm, gain, kept, state)


def memory_of(coef, k, ko, v, norm, kept, state):
    return pl.pallas_call(
        memory_kernel,
        in_specs=[VMEM] * 6 + [ANY],
        out_specs=(ANY, VMEM, VMEM),
        out_shape=(
            jax.ShapeDtypeStruct((ITEMS, DK, DV), jnp.float32),
            jax.ShapeDtypeStruct((ITEMS, DK), jnp.float32),
            jax.ShapeDtypeStruct((HEADS, SEQS), jnp.float32),
        ),
        scratch_shapes=[
            pltpu.VMEM((ITEMS - KEPT, DK, DV), jnp.float32),
            pltpu.VMEM((ITEMS, DK, DV), jnp.float32),
            pltpu.SemaphoreType.DMA((CHUNKS,)),
            pltpu.SemaphoreType.DMA((CHUNKS,)),
        ],
        name="memory",
    )(coef, k, ko, v, norm, kept, state)


def front_kernel(block_hbm, *refs):
    count = (len(refs) - 4) // 2
    inputs, pieces_hbm, outputs = refs[:count], refs[count], refs[count + 1 : 2 * count + 1]
    block, pieces, sems = refs[2 * count + 1 :]
    first = pltpu.make_async_copy(block_hbm, block, sems.at[0])
    first.start()
    copies = [
        pltpu.make_async_copy(src.at[pl.ds(0, dst.shape[0])], dst, sems.at[i + 2])
        for i, (src, dst) in enumerate(zip(inputs, outputs, strict=True))
    ]
    for copy in copies:
        copy.start()
    first.wait()
    for i in range(pieces.shape[0]):
        pieces[i] = block[...]
    last = pltpu.make_async_copy(pieces, pieces_hbm, sems.at[1])
    last.start()
    for copy in copies:
        copy.wait()
    last.wait()


def front(block, count, arrays, state):
    shape = (count, *block.shape)
    outs = [pltpu.VMEM(a.shape, a.dtype) for a in arrays]
    outs.append(pltpu.VMEM((KEPT, *state.shape[1:]), state.dtype))
    return pl.pallas_call(
        front_kernel,
        in_specs=[ANY] * (1 + len(outs)),
        out_specs=[ANY] + [VMEM] * len(outs),
        out_shape=[jax.ShapeDtypeStruct(shape, block.dtype), *outs],
        scratch_shapes=[
            pltpu.VMEM(block.shape, block.dtype),
            pltpu.VMEM(shape, block.dtype),
            pltpu.SemaphoreType.DMA((2 + len(outs),)),
        ],
        name="front",
    )(block, *arrays, state)


def product_kernel(rows_ref, weight_ref, out_ref, *, order):
    terms = dot_bt(rows_ref[...], weight_ref[...]).astype(jnp.bfloat16)
    for i, source in enumerate(order):
        out_ref[i] = terms[source * SEQS : (source + 1) * SEQS]


def product(rows, weight, order):
    return pl.pallas_call(
        functools.partial(product_kernel, order=order),
        in_specs=[VMEM, VMEM],
        out_specs=VMEM,
        out_shape=pltpu.VMEM((len(order), SEQS, weight.shape[0]), jnp.bfloat16),
        name="product",
    )(rows, weight)


def join_kernel(terms_ref, out_ref, *, order, tps, block):
    cross = len(order) // tps
    slot = {source: i for i, source in enumerate(order)}
    planes = out_ref.shape[1] // DK
    lane = iota((SEQS, DK), 1) // block
    for part in range(terms_ref.shape[2] // DK):
        cols = slice(part * DK, (part + 1) * DK)
        sums = [
            sum(terms_ref[slot[g * tps + t], :, cols].astype(jnp.float32) for t in range(tps))
            for g in range(cross)
        ]
        step = 1
        while step < cross:
            low = lane & step == 0
            swapped = list(sums)
            for g in range(cross):
                if g & step == 0:
                    a, b = sums[g], sums[g + step]
                    swapped[g] = jnp.where(low, a, pltpu.roll(b, step * block, 1))
                    swapped[g + step] = jnp.where(low, pltpu.roll(a, DK - step * block, 1), b)
            sums = swapped
            step *= 2
        for z in range(cross):
            at = (FIRST_Z + part * cross + z) % planes * DK
            out_ref[:, at : at + DK] = sums[z].astype(jnp.bfloat16)


def joined(terms, order, tps, block):
    sources, seqs, cols = terms.shape
    return pl.pallas_call(
        functools.partial(join_kernel, order=order, tps=tps, block=block),
        in_specs=[VMEM],
        out_specs=VMEM,
        out_shape=jax.ShapeDtypeStruct((seqs, sources // tps * cols), jnp.bfloat16),
        name="join",
    )(terms)


def exchanged(pieces, axes, order):
    return lax.all_to_all(
        pieces, axes, split_axis=0, concat_axis=0, tiled=True, axis_index_groups=[order]
    )


def from_place(first, size):
    return [(first + i) % size for i in range(size)]


def in_vmem(array):
    return pltpu.with_memory_space_constraint(array, pltpu.VMEM)


def on_device(
    queries,
    keys,
    values,
    in_gate,
    forget_pre,
    old_keys,
    old_values,
    old_in_gate,
    old_forget,
    accepted,
    state_mem,
    state_norm,
    state_max,
    norm_gain,
    out_weight,
):
    zs, cross, tps = lax.axis_size("kv_0"), lax.axis_size(PLANE), lax.axis_size("tp")
    q, k, ko = (a.reshape(ROWS, DK) for a in (queries, keys, old_keys))
    v, vo = (
        a.reshape(SEQS, PROPS, HEADS, 2, DK).swapaxes(2, 3).reshape(RUN, DK)
        for a in (values, old_values)
    )
    gates = (
        a.transpose(1, 2, 0) for a in (in_gate, forget_pre, old_in_gate, old_forget)
    )
    norm = state_norm.reshape(ITEMS, DK)
    state = state_mem.reshape(ITEMS, DK, DV)
    inputs = (q, k, ko, v, vo, *gates, accepted[None], state_max.T, norm, norm_gain)
    pieces, *inputs = front(out_weight.T, zs, inputs, state)
    inputs = [in_vmem(a) for a in inputs]
    q, k, ko, *_, norm, _, kept = inputs
    weight = exchanged(pieces, "kv_0", from_place(FIRST_Z, zs))
    weight = weight.reshape(-1, out_weight.shape[0])
    hidden, coef, run_values = hidden_of(*inputs, state)
    rows = lax.all_gather(hidden.reshape(PROPS * SEQS, -1), PLANE, tiled=True)
    order = [g * tps + t for g in from_place(FIRST_CROSS, cross) for t in from_place(FIRST_TP, tps)]
    terms = product(in_vmem(rows), in_vmem(weight), order)
    terms = exchanged(terms, (*PLANE, "tp"), order)
    new_mem, new_norm, new_max = memory_of(
        in_vmem(coef), k, ko, in_vmem(run_values), norm, kept, state
    )
    mixed = joined(in_vmem(terms), order, tps, out_weight.shape[1])[:, None]
    return (
        mixed,
        new_mem.reshape(state_mem.shape),
        new_norm.reshape(state_norm.shape),
        new_max.T,
    )


def solution(mesh):
    finer = Mesh(mesh.devices.reshape(16, 4, 2, mesh.shape["tp"]), (*KV, "tp"))
    in_specs = (
        P(KV, None, "tp", None),
        P(KV, None, "tp", None),
        P(KV, None, "tp", None),
        P(KV, None, "tp"),
        P(KV, None, "tp"),
        P(KV, None, "tp", None),
        P(KV, None, "tp", None),
        P(KV, None, "tp"),
        P(KV, None, "tp"),
        P(KV),
        P(KV, "tp", None, None),
        P(KV, "tp", None),
        P(KV, "tp"),
        P("tp", None),
        P("tp", KV),
    )
    out_specs = (P(KV, "tp", None), P(KV, "tp", None, None), P(KV, "tp", None), P(KV, "tp"))
    return jax.shard_map(
        on_device, mesh=finer, in_specs=in_specs, out_specs=out_specs, check_vma=False
    )
```

```python
import functools

import jax
import jax.numpy as jnp
from jax import lax
from jax.experimental import pallas as pl
from jax.experimental.pallas import tpu as pltpu
from jax.sharding import Mesh
from jax.sharding import PartitionSpec as P

KV = ("kv_0", "kv_1", "kv_2")
PLANE = ("kv_1", "kv_2")

SEQS = 8
PROPS = 4
HEADS = 2
DK = 128
DV = 256
ROWS = SEQS * PROPS * HEADS
RUN = 2 * ROWS
ITEMS = SEQS * HEADS
CHUNK = 4
CHUNKS = ITEMS // CHUNK
KEPT = 16
EPS = 1e-5
FIRST_Z, FIRST_CROSS, FIRST_TP = 12, 5, 2


def iota(shape, dim):
    return lax.broadcasted_iota(jnp.int32, shape, dim)


def item_of(row):
    return (row // 8) % 8 * 2 + row % 2


def place_of(row):
    return row // 64 * 4 + row // 2 % 4


def exact_dot(a, b):
    return jnp.dot(a, b, precision=lax.Precision.HIGHEST, preferred_element_type=jnp.float32)


def halves(x):
    high = x.astype(jnp.bfloat16)
    return high, (x - high.astype(jnp.float32)).astype(jnp.bfloat16)


def dot_bt(a, b):
    return lax.dot_general(a, b, (((1,), (1,)), ((), ())), preferred_element_type=jnp.float32)


def log_sigmoid(x):
    return jnp.minimum(x, 0.0) - jnp.log1p(jnp.exp(-jnp.abs(x)))


def in_row_order(view):
    dst, src = iota((RUN, RUN), 0), iota((RUN, RUN), 1)
    row = dst % ROWS
    pick = src == row // 2 * 4 + dst // ROWS * 2 + row % 2
    rows = jnp.dot(pick.astype(jnp.bfloat16), view, preferred_element_type=jnp.float32)
    return jnp.concatenate([rows[:ROWS], rows[ROWS:]], axis=1).astype(jnp.bfloat16)


def state_copies(state_hbm, rest, sems):
    return [
        pltpu.make_async_copy(
            state_hbm.at[pl.ds(KEPT + i * CHUNK, CHUNK)], part, sems.at[i]
        )
        for i, part in enumerate(rest)
    ]


def hidden_kernel(
    q_ref, k_ref, ko_ref, v_ref, vo_ref, ig_ref, fg_ref, igo_ref, fgo_ref, acc_ref, smax_ref,
    norm_ref, gain_ref, *refs,
):
    kept = refs[: KEPT // CHUNK]
    state_hbm, hidden_ref, coef_ref, values_ref, *rest, flat, sems = refs[KEPT // CHUNK :]
    copies = state_copies(state_hbm, rest, sems)
    for copy in copies:
        copy.start()

    lane1 = iota((1, RUN), 1)
    parts = []
    for ref in (igo_ref, ig_ref, fgo_ref, fg_ref):
        parts.append(jnp.concatenate([ref[p] for p in range(PROPS)], axis=0))
    parts.append(
        jnp.concatenate(
            [smax_ref[...], acc_ref[...].astype(jnp.float32), jnp.zeros((5, SEQS), jnp.float32)],
            axis=0,
        )
    )
    spread = (iota((SEQS, RUN), 1) % 64 // 8 == iota((SEQS, RUN), 0)).astype(jnp.float32)
    wide = exact_dot(jnp.concatenate(parts, axis=0), spread)
    own = iota((8, RUN), 0) == iota((8, RUN), 1) % 8
    rows = [
        jnp.sum(jnp.where(own, wide[8 * a : 8 * a + 8], 0.0), axis=0, keepdims=True)
        for a in range(4)
    ]
    smax = jnp.where(lane1 % 2 == 0, wide[32:33], wide[33:34])
    old = lane1 < ROWS
    live = (lane1 // 2 % 4).astype(jnp.float32) < wide[34:35]
    ig = jnp.where(old, jnp.where(live, rows[0], -jnp.inf), rows[1])
    forget = log_sigmoid(jnp.where(old, rows[2], rows[3]))
    forget = jnp.where(old & ~live, 0.0, forget)

    src, dst = iota((RUN, RUN), 0), iota((RUN, RUN), 1)
    together = item_of(src) == item_of(dst)
    upto = (together & (place_of(src) <= place_of(dst))).astype(jnp.float32)
    sums = exact_dot(
        jnp.broadcast_to(forget, (8, RUN)),
        jnp.concatenate([upto, together.astype(jnp.float32)], axis=1),
    )
    b = sums[0:1, :RUN]
    b_last = sums[0:1, RUN:]

    qrow, lane = iota((ROWS, RUN), 0), iota((ROWS, RUN), 1)
    same = item_of(qrow) == item_of(lane)
    valid = same & (place_of(lane) <= PROPS + qrow // 2 % 4)
    at = lane == ROWS + qrow
    b_col = jnp.sum(jnp.where(at, b, 0.0), axis=1, keepdims=True)
    inter = jnp.sum(jnp.where(at, b + smax, 0.0), axis=1, keepdims=True)
    logd = jnp.where(valid, b_col + (ig - b), -jnp.inf)
    m_row = jnp.maximum(inter, jnp.max(logd, axis=1, keepdims=True))
    decay = jnp.exp(logd - m_row)
    w_inter = jnp.exp(inter - m_row)

    last = same & (qrow // 2 % 4 == PROPS - 1)
    new_max = jnp.sum(jnp.where(last, m_row, 0.0), axis=0, keepdims=True)
    coef_ref[0:1, :] = jnp.exp(b_last - b + ig - new_max)
    coef_ref[1:2, :] = jnp.exp(b_last + smax - new_max)
    coef_ref[2:3, :] = new_max
    coef_ref[3:8, :] = jnp.zeros((5, RUN), jnp.float32)

    scale = DK**-0.5
    q = q_ref[...]
    k = jnp.concatenate([ko_ref[...], k_ref[...]], axis=0)
    v = jnp.concatenate([in_row_order(vo_ref[...]), in_row_order(v_ref[...])], axis=0)
    values_ref[...] = v
    probs = dot_bt(q, k) * scale * decay
    p_high, p_low = halves(probs)
    intra = jnp.dot(p_high, v, preferred_element_type=jnp.float32) + jnp.dot(
        p_low, v, preferred_element_type=jnp.float32
    )
    qn = lax.dot_general(
        q.astype(jnp.float32), norm_ref[...], (((1,), (1,)), ((), ())),
        precision=lax.Precision.HIGHEST, preferred_element_type=jnp.float32,
    )
    mine = item_of(iota((ROWS, ITEMS), 0)) == iota((ROWS, ITEMS), 1)
    qn = jnp.sum(jnp.where(mine, qn, 0.0), axis=1, keepdims=True)
    w_scaled = w_inter * scale
    den = w_scaled * qn + jnp.sum(probs, axis=1, keepdims=True)
    inv = 1.0 / jnp.maximum(jnp.abs(den), 1.0)
    gain = jnp.where(iota((ROWS // CHUNKS, DV), 0) % 2 == 0, gain_ref[0:1, :], gain_ref[1:2, :])

    for copy in copies:
        copy.wait()
    size = ROWS // CHUNKS
    for c in range(CHUNKS):
        lo, hi = c * size, (c + 1) * size
        qc = q[lo:hi].astype(jnp.float32)
        item = item_of(iota((size, DK), 0) + lo)
        lhs = jnp.concatenate(
            [jnp.where(item == c * CHUNK + i, qc, 0.0) for i in range(CHUNK)], axis=1
        ).astype(jnp.bfloat16)
        s_high, s_low = halves((*kept, *rest)[c][...].reshape(CHUNK * DK, DV))
        num = jnp.dot(lhs, s_high, preferred_element_type=jnp.float32) + jnp.dot(
            lhs, s_low, preferred_element_type=jnp.float32
        )
        h = (w_scaled[lo:hi] * num + intra[lo:hi]) * inv[lo:hi]
        h = h - jnp.mean(h, axis=1, keepdims=True)
        var = jnp.mean(h * h, axis=1, keepdims=True)
        h = h * lax.rsqrt(var + EPS) * gain
        for half in range(2):
            flat[half, lo:hi, :] = h[:, half * DK : (half + 1) * DK]
    for p in range(PROPS):
        for head in range(HEADS):
            for half in range(2):
                piece = flat[half, pl.ds(p * HEADS + head, SEQS, stride=8), :]
                at = head * DV + half * DK
                hidden_ref[p, :, at : at + DK] = piece.astype(jnp.bfloat16)


def memory_kernel(
    coef_ref, k_ref, ko_ref, values_ref, norm_ref, *refs,
):
    kept = refs[: KEPT // CHUNK]
    state_hbm, new_hbm, new_norm_hbm, new_max_hbm, *rest = refs[KEPT // CHUNK :]
    *rest, new, new_norm_ref, new_max_ref, sems, out_sems = rest
    copies = state_copies(state_hbm, rest, sems)
    for copy in copies:
        copy.start()
    tok, keep = coef_ref[0:1, :], coef_ref[1:2, :]
    k = jnp.concatenate([ko_ref[...], k_ref[...]], axis=0).astype(jnp.float32)
    v = values_ref[...]
    lane = iota((8, RUN), 1)
    first = (place_of(lane) == 0) & (lane % 2 == iota((8, RUN), 0))
    seq = (iota((RUN, SEQS), 0) // 8 % 8 == iota((RUN, SEQS), 1)).astype(jnp.float32)
    new_max_ref[...] = exact_dot(jnp.where(first, coef_ref[2:3, :], 0.0), seq)[:HEADS]
    lane = iota((ITEMS, RUN), 1)
    mine = item_of(lane) == iota((ITEMS, RUN), 0)
    t_high, t_low = halves(jnp.where(mine, tok, 0.0))
    kb = k.astype(jnp.bfloat16)
    share = jnp.sum(jnp.where(mine & (place_of(lane) == 0), keep, 0.0), axis=1, keepdims=True)
    new_norm_ref[...] = (
        share * norm_ref[...]
        + jnp.dot(t_high, kb, preferred_element_type=jnp.float32)
        + jnp.dot(t_low, kb, preferred_element_type=jnp.float32)
    )
    stores = [
        pltpu.make_async_copy(src, dst, out_sems.at[CHUNKS + i])
        for i, (src, dst) in enumerate(
            ((new_norm_ref, new_norm_hbm), (new_max_ref, new_max_hbm))
        )
    ]
    for store in stores:
        store.start()
    high, low = halves(k.T * tok)
    both = jnp.concatenate([high, low], axis=1)
    twice = jnp.concatenate([v, v], axis=0)
    lane = item_of(iota((8, 2 * RUN), 1) % RUN)
    for c in range(CHUNKS):
        if c * CHUNK >= KEPT:
            copies[c - KEPT // CHUNK].wait()
        for i in range(c * CHUNK, (c + 1) * CHUNK):
            mask = (lane == i).astype(jnp.float32)[:1].astype(jnp.bfloat16)
            update = jnp.dot(both * mask, twice, preferred_element_type=jnp.float32)
            at = i // 2 * 8 + i % 2
            new[i] = keep[:, at : at + 1] * (*kept, *rest)[c][i - c * CHUNK] + update
        stores.append(
            pltpu.make_async_copy(
                new.at[pl.ds(c * CHUNK, CHUNK)], new_hbm.at[pl.ds(c * CHUNK, CHUNK)], out_sems.at[c]
            )
        )
        stores[-1].start()
    for store in stores:
        store.wait()


VMEM = pl.BlockSpec(memory_space=pltpu.VMEM)
ANY = pl.BlockSpec(memory_space=pl.ANY)


def hidden_of(q, k, ko, v, vo, ig, fg, igo, fgo, accepted, smax, norm, gain, *kept, state):
    return pl.pallas_call(
        hidden_kernel,
        in_specs=[VMEM] * (13 + len(kept)) + [ANY],
        out_specs=(VMEM, VMEM, VMEM),
        out_shape=(
            pltpu.VMEM((PROPS, SEQS, HEADS * DV), jnp.bfloat16),
            pltpu.VMEM((8, RUN), jnp.float32),
            pltpu.VMEM((RUN, DV), jnp.bfloat16),
        ),
        scratch_shapes=[
            *[pltpu.VMEM((CHUNK, DK, DV), jnp.float32)] * ((ITEMS - KEPT) // CHUNK),
            pltpu.VMEM((2, ROWS, DK), jnp.float32),
            pltpu.SemaphoreType.DMA((CHUNKS,)),
        ],
        name="hidden",
    )(q, k, ko, v, vo, ig, fg, igo, fgo, accepted, smax, norm, gain, *kept, state)


def memory_of(coef, k, ko, v, norm, *kept, state):
    return pl.pallas_call(
        memory_kernel,
        in_specs=[VMEM] * (5 + len(kept)) + [ANY],
        out_specs=(ANY, ANY, ANY),
        out_shape=(
            jax.ShapeDtypeStruct((ITEMS, DK, DV), jnp.float32),
            jax.ShapeDtypeStruct((ITEMS, DK), jnp.float32),
            jax.ShapeDtypeStruct((HEADS, SEQS), jnp.float32),
        ),
        scratch_shapes=[
            *[pltpu.VMEM((CHUNK, DK, DV), jnp.float32)] * ((ITEMS - KEPT) // CHUNK),
            pltpu.VMEM((ITEMS, DK, DV), jnp.float32),
            pltpu.VMEM((ITEMS, DK), jnp.float32),
            pltpu.VMEM((HEADS, SEQS), jnp.float32),
            pltpu.SemaphoreType.DMA((CHUNKS,)),
            pltpu.SemaphoreType.DMA((CHUNKS + 2,)),
        ],
        name="memory",
    )(coef, k, ko, v, norm, *kept, state)


def front_kernel(block_hbm, *refs):
    *refs, block, pieces, sems = refs
    count = (len(refs) - 2 - KEPT // CHUNK) // 2
    inputs, state_hbm, pieces_hbm, outputs = (
        refs[:count], refs[count], refs[count + 1], refs[count + 2 :]
    )
    first = pltpu.make_async_copy(block_hbm, block, sems.at[0])
    first.start()
    copies = [
        pltpu.make_async_copy(src, dst, sems.at[i + 2])
        for i, (src, dst) in enumerate(zip(inputs, outputs))
    ]
    copies += [
        pltpu.make_async_copy(
            state_hbm.at[pl.ds(i * CHUNK, CHUNK)], dst, sems.at[len(inputs) + i + 2]
        )
        for i, dst in enumerate(outputs[len(inputs) :])
    ]
    for copy in copies:
        copy.start()
    first.wait()
    for i in range(pieces.shape[0]):
        pieces[i] = block[...]
    last = pltpu.make_async_copy(pieces, pieces_hbm, sems.at[1])
    last.start()
    for copy in copies:
        copy.wait()
    last.wait()


def front(block, count, arrays, state):
    shape = (count, *block.shape)
    outs = [pltpu.VMEM(a.shape, a.dtype) for a in arrays]
    outs += [pltpu.VMEM((CHUNK, *state.shape[1:]), state.dtype)] * (KEPT // CHUNK)
    return pl.pallas_call(
        front_kernel,
        in_specs=[ANY] * (2 + len(arrays)),
        out_specs=[ANY] + [VMEM] * len(outs),
        out_shape=[jax.ShapeDtypeStruct(shape, block.dtype), *outs],
        scratch_shapes=[
            pltpu.VMEM(block.shape, block.dtype),
            pltpu.VMEM(shape, block.dtype),
            pltpu.SemaphoreType.DMA((2 + len(outs),)),
        ],
        name="front",
    )(block, *arrays, state)


def product_kernel(rows_ref, weight_ref, out_ref, *, order):
    terms = dot_bt(rows_ref[...], weight_ref[...]).astype(jnp.bfloat16)
    for i, source in enumerate(order):
        out_ref[i] = terms[source * SEQS : (source + 1) * SEQS]


def product(rows, weight, order):
    return pl.pallas_call(
        functools.partial(product_kernel, order=order),
        in_specs=[VMEM, VMEM],
        out_specs=VMEM,
        out_shape=pltpu.VMEM((len(order), SEQS, weight.shape[0]), jnp.bfloat16),
        name="product",
    )(rows, weight)


def join_kernel(terms_ref, out_ref, *, order, tps, block):
    cross = len(order) // tps
    slot = {source: i for i, source in enumerate(order)}
    planes = out_ref.shape[1] // DK
    lane = iota((SEQS, DK), 1) // block
    for part in range(terms_ref.shape[2] // DK):
        cols = slice(part * DK, (part + 1) * DK)
        sums = [
            sum(terms_ref[slot[g * tps + t], :, cols].astype(jnp.float32) for t in range(tps))
            for g in range(cross)
        ]
        step = 1
        while step < cross:
            low = lane & step == 0
            swapped = list(sums)
            for g in range(cross):
                if g & step == 0:
                    a, b = sums[g], sums[g + step]
                    swapped[g] = jnp.where(low, a, pltpu.roll(b, step * block, 1))
                    swapped[g + step] = jnp.where(low, pltpu.roll(a, DK - step * block, 1), b)
            sums = swapped
            step *= 2
        for z in range(cross):
            at = (FIRST_Z + part * cross + z) % planes * DK
            out_ref[:, at : at + DK] = sums[z].astype(jnp.bfloat16)


def joined(terms, order, tps, block):
    sources, seqs, cols = terms.shape
    return pl.pallas_call(
        functools.partial(join_kernel, order=order, tps=tps, block=block),
        in_specs=[VMEM],
        out_specs=VMEM,
        out_shape=jax.ShapeDtypeStruct((seqs, sources // tps * cols), jnp.bfloat16),
        name="join",
    )(terms)


def exchanged(pieces, axes, order):
    return lax.all_to_all(
        pieces, axes, split_axis=0, concat_axis=0, tiled=True, axis_index_groups=[order]
    )


def from_place(first, size):
    return [(first + i) % size for i in range(size)]


def in_vmem(array):
    return pltpu.with_memory_space_constraint(array, pltpu.VMEM)


def on_device(
    queries,
    keys,
    values,
    in_gate,
    forget_pre,
    old_keys,
    old_values,
    old_in_gate,
    old_forget,
    accepted,
    state_mem,
    state_norm,
    state_max,
    norm_gain,
    out_weight,
):
    zs, cross, tps = lax.axis_size("kv_0"), lax.axis_size(PLANE), lax.axis_size("tp")
    q, k, ko = (a.reshape(ROWS, DK) for a in (queries, keys, old_keys))
    v, vo = (
        a.reshape(SEQS, PROPS, HEADS, 2, DK).swapaxes(2, 3).reshape(RUN, DK)
        for a in (values, old_values)
    )
    gates = (
        a.transpose(1, 2, 0) for a in (in_gate, forget_pre, old_in_gate, old_forget)
    )
    norm = state_norm.reshape(ITEMS, DK)
    state = state_mem.reshape(ITEMS, DK, DV)
    inputs = (q, k, ko, v, vo, *gates, accepted[None], state_max.T, norm, norm_gain)
    pieces, *inputs = front(out_weight.T, zs, inputs, state)
    inputs = [in_vmem(a) for a in inputs]
    q, k, ko = inputs[:3]
    norm, kept = inputs[11], inputs[13:]
    weight = exchanged(pieces, "kv_0", from_place(FIRST_Z, zs))
    weight = weight.reshape(-1, out_weight.shape[0])
    hidden, coef, run_values = hidden_of(*inputs, state=state)
    rows = lax.all_gather(hidden.reshape(PROPS * SEQS, -1), PLANE, tiled=True)
    order = [g * tps + t for g in from_place(FIRST_CROSS, cross) for t in from_place(FIRST_TP, tps)]
    terms = product(in_vmem(rows), in_vmem(weight), order)
    terms = exchanged(terms, (*PLANE, "tp"), order)
    new_mem, new_norm, new_max = memory_of(
        in_vmem(coef), k, ko, in_vmem(run_values), norm, *kept, state=state
    )
    mixed = joined(in_vmem(terms), order, tps, out_weight.shape[1])[:, None]
    return (
        mixed,
        new_mem.reshape(state_mem.shape),
        new_norm.reshape(state_norm.shape),
        new_max.T,
    )


def solution(mesh):
    finer = Mesh(mesh.devices.reshape(16, 4, 2, mesh.shape["tp"]), (*KV, "tp"))
    in_specs = (
        P(KV, None, "tp", None),
        P(KV, None, "tp", None),
        P(KV, None, "tp", None),
        P(KV, None, "tp"),
        P(KV, None, "tp"),
        P(KV, None, "tp", None),
        P(KV, None, "tp", None),
        P(KV, None, "tp"),
        P(KV, None, "tp"),
        P(KV),
        P(KV, "tp", None, None),
        P(KV, "tp", None),
        P(KV, "tp"),
        P("tp", None),
        P("tp", KV),
    )
    out_specs = (P(KV, "tp", None), P(KV, "tp", None, None), P(KV, "tp", None), P(KV, "tp"))
    return jax.shard_map(
        on_device, mesh=finer, in_specs=in_specs, out_specs=out_specs, check_vma=False
    )
```

```python
import functools

import jax
import jax.numpy as jnp
from jax import lax
from jax.experimental import pallas as pl
from jax.experimental.pallas import tpu as pltpu
from jax.sharding import Mesh
from jax.sharding import PartitionSpec as P

KV = ("kv_0", "kv_1", "kv_2")
PLANE = ("kv_1", "kv_2")

SEQS = 8
PROPS = 4
HEADS = 2
DK = 128
DV = 256
ROWS = SEQS * PROPS * HEADS
RUN = 2 * ROWS
ITEMS = SEQS * HEADS
CHUNK = 4
CHUNKS = ITEMS // CHUNK
KEPT = 16
EPS = 1e-5
Z_ORDER = (12, 0, 15, 1, 14, 2, 13, 3, 4, 5, 6, 7, 8, 9, 10, 11)
FIRST_CROSS, FIRST_TP = 5, 2


def iota(shape, dim):
    return lax.broadcasted_iota(jnp.int32, shape, dim)


def item_of(row):
    return (row // 8) % 8 * 2 + row % 2


def place_of(row):
    return row // 64 * 4 + row // 2 % 4


def exact_dot(a, b):
    return jnp.dot(a, b, precision=lax.Precision.HIGHEST, preferred_element_type=jnp.float32)


def halves(x):
    high = x.astype(jnp.bfloat16)
    return high, (x - high.astype(jnp.float32)).astype(jnp.bfloat16)


def dot_bt(a, b):
    return lax.dot_general(a, b, (((1,), (1,)), ((), ())), preferred_element_type=jnp.float32)


def log_sigmoid(x):
    return jnp.minimum(x, 0.0) - jnp.log1p(jnp.exp(-jnp.abs(x)))


def in_row_order(view):
    dst, src = iota((RUN, RUN), 0), iota((RUN, RUN), 1)
    row = dst % ROWS
    pick = src == row // 2 * 4 + dst // ROWS * 2 + row % 2
    rows = jnp.dot(pick.astype(jnp.bfloat16), view, preferred_element_type=jnp.float32)
    return jnp.concatenate([rows[:ROWS], rows[ROWS:]], axis=1).astype(jnp.bfloat16)


def state_copies(state_hbm, rest, sems):
    return [
        pltpu.make_async_copy(
            state_hbm.at[pl.ds(KEPT + i * CHUNK, CHUNK)], part, sems.at[i]
        )
        for i, part in enumerate(rest)
    ]


def hidden_kernel(
    q_ref, k_ref, ko_ref, v_ref, vo_ref, ig_ref, fg_ref, igo_ref, fgo_ref, acc_ref, smax_ref,
    norm_ref, gain_ref, *refs,
):
    kept = refs[: KEPT // CHUNK]
    state_hbm, hidden_ref, coef_ref, values_ref, *rest, flat, sems = refs[KEPT // CHUNK :]
    copies = state_copies(state_hbm, rest, sems)
    for copy in copies:
        copy.start()

    lane1 = iota((1, RUN), 1)
    parts = []
    for ref in (igo_ref, ig_ref, fgo_ref, fg_ref):
        parts.append(jnp.concatenate([ref[p] for p in range(PROPS)], axis=0))
    parts.append(
        jnp.concatenate(
            [smax_ref[...], acc_ref[...].astype(jnp.float32), jnp.zeros((5, SEQS), jnp.float32)],
            axis=0,
        )
    )
    spread = (iota((SEQS, RUN), 1) % 64 // 8 == iota((SEQS, RUN), 0)).astype(jnp.float32)
    wide = exact_dot(jnp.concatenate(parts, axis=0), spread)
    own = iota((8, RUN), 0) == iota((8, RUN), 1) % 8
    rows = [
        jnp.sum(jnp.where(own, wide[8 * a : 8 * a + 8], 0.0), axis=0, keepdims=True)
        for a in range(4)
    ]
    smax = jnp.where(lane1 % 2 == 0, wide[32:33], wide[33:34])
    old = lane1 < ROWS
    live = (lane1 // 2 % 4).astype(jnp.float32) < wide[34:35]
    ig = jnp.where(old, jnp.where(live, rows[0], -jnp.inf), rows[1])
    forget = log_sigmoid(jnp.where(old, rows[2], rows[3]))
    forget = jnp.where(old & ~live, 0.0, forget)

    src, dst = iota((RUN, RUN), 0), iota((RUN, RUN), 1)
    together = item_of(src) == item_of(dst)
    upto = (together & (place_of(src) <= place_of(dst))).astype(jnp.float32)
    sums = exact_dot(
        jnp.broadcast_to(forget, (8, RUN)),
        jnp.concatenate([upto, together.astype(jnp.float32)], axis=1),
    )
    b = sums[0:1, :RUN]
    b_last = sums[0:1, RUN:]

    qrow, lane = iota((ROWS, RUN), 0), iota((ROWS, RUN), 1)
    same = item_of(qrow) == item_of(lane)
    valid = same & (place_of(lane) <= PROPS + qrow // 2 % 4)
    at = lane == ROWS + qrow
    b_col = jnp.sum(jnp.where(at, b, 0.0), axis=1, keepdims=True)
    inter = jnp.sum(jnp.where(at, b + smax, 0.0), axis=1, keepdims=True)
    logd = jnp.where(valid, b_col + (ig - b), -jnp.inf)
    m_row = jnp.maximum(inter, jnp.max(logd, axis=1, keepdims=True))
    decay = jnp.exp(logd - m_row)
    w_inter = jnp.exp(inter - m_row)

    last = same & (qrow // 2 % 4 == PROPS - 1)
    new_max = jnp.sum(jnp.where(last, m_row, 0.0), axis=0, keepdims=True)
    coef_ref[0:1, :] = jnp.exp(b_last - b + ig - new_max)
    coef_ref[1:2, :] = jnp.exp(b_last + smax - new_max)
    coef_ref[2:3, :] = new_max
    coef_ref[3:8, :] = jnp.zeros((5, RUN), jnp.float32)

    scale = DK**-0.5
    q = q_ref[...]
    k = jnp.concatenate([ko_ref[...], k_ref[...]], axis=0)
    v = jnp.concatenate([in_row_order(vo_ref[...]), in_row_order(v_ref[...])], axis=0)
    values_ref[...] = v
    probs = dot_bt(q, k) * scale * decay
    p_high, p_low = halves(probs)
    intra = jnp.dot(p_high, v, preferred_element_type=jnp.float32) + jnp.dot(
        p_low, v, preferred_element_type=jnp.float32
    )
    qn = lax.dot_general(
        q.astype(jnp.float32), norm_ref[...], (((1,), (1,)), ((), ())),
        precision=lax.Precision.HIGHEST, preferred_element_type=jnp.float32,
    )
    mine = item_of(iota((ROWS, ITEMS), 0)) == iota((ROWS, ITEMS), 1)
    qn = jnp.sum(jnp.where(mine, qn, 0.0), axis=1, keepdims=True)
    w_scaled = w_inter * scale
    den = w_scaled * qn + jnp.sum(probs, axis=1, keepdims=True)
    inv = 1.0 / jnp.maximum(jnp.abs(den), 1.0)
    gain = jnp.where(iota((ROWS // CHUNKS, DV), 0) % 2 == 0, gain_ref[0:1, :], gain_ref[1:2, :])

    for copy in copies:
        copy.wait()
    size = ROWS // CHUNKS
    for c in range(CHUNKS):
        lo, hi = c * size, (c + 1) * size
        qc = q[lo:hi].astype(jnp.float32)
        item = item_of(iota((size, DK), 0) + lo)
        lhs = jnp.concatenate(
            [jnp.where(item == c * CHUNK + i, qc, 0.0) for i in range(CHUNK)], axis=1
        ).astype(jnp.bfloat16)
        s_high, s_low = halves((*kept, *rest)[c][...].reshape(CHUNK * DK, DV))
        num = jnp.dot(lhs, s_high, preferred_element_type=jnp.float32) + jnp.dot(
            lhs, s_low, preferred_element_type=jnp.float32
        )
        h = (w_scaled[lo:hi] * num + intra[lo:hi]) * inv[lo:hi]
        h = h - jnp.mean(h, axis=1, keepdims=True)
        var = jnp.mean(h * h, axis=1, keepdims=True)
        h = h * lax.rsqrt(var + EPS) * gain
        for half in range(2):
            flat[half, lo:hi, :] = h[:, half * DK : (half + 1) * DK]
    for p in range(PROPS):
        for head in range(HEADS):
            for half in range(2):
                piece = flat[half, pl.ds(p * HEADS + head, SEQS, stride=8), :]
                at = head * DV + half * DK
                hidden_ref[p, :, at : at + DK] = piece.astype(jnp.bfloat16)


def memory_kernel(
    coef_ref, k_ref, ko_ref, values_ref, norm_ref, *refs,
):
    kept = refs[: KEPT // CHUNK]
    state_hbm, new_hbm, new_norm_hbm, new_max_hbm, *rest = refs[KEPT // CHUNK :]
    *rest, new, new_norm_ref, new_max_ref, sems, out_sems = rest
    copies = state_copies(state_hbm, rest, sems)
    for copy in copies:
        copy.start()
    tok, keep = coef_ref[0:1, :], coef_ref[1:2, :]
    k = jnp.concatenate([ko_ref[...], k_ref[...]], axis=0).astype(jnp.float32)
    v = values_ref[...]
    lane = iota((8, RUN), 1)
    first = (place_of(lane) == 0) & (lane % 2 == iota((8, RUN), 0))
    seq = (iota((RUN, SEQS), 0) // 8 % 8 == iota((RUN, SEQS), 1)).astype(jnp.float32)
    new_max_ref[...] = exact_dot(jnp.where(first, coef_ref[2:3, :], 0.0), seq)[:HEADS]
    lane = iota((ITEMS, RUN), 1)
    mine = item_of(lane) == iota((ITEMS, RUN), 0)
    t_high, t_low = halves(jnp.where(mine, tok, 0.0))
    kb = k.astype(jnp.bfloat16)
    share = jnp.sum(jnp.where(mine & (place_of(lane) == 0), keep, 0.0), axis=1, keepdims=True)
    new_norm_ref[...] = (
        share * norm_ref[...]
        + jnp.dot(t_high, kb, preferred_element_type=jnp.float32)
        + jnp.dot(t_low, kb, preferred_element_type=jnp.float32)
    )
    stores = [
        pltpu.make_async_copy(src, dst, out_sems.at[CHUNKS + i])
        for i, (src, dst) in enumerate(
            ((new_norm_ref, new_norm_hbm), (new_max_ref, new_max_hbm))
        )
    ]
    for store in stores:
        store.start()
    high, low = halves(k.T * tok)
    both = jnp.concatenate([high, low], axis=1)
    twice = jnp.concatenate([v, v], axis=0)
    lane = item_of(iota((8, 2 * RUN), 1) % RUN)
    for c in range(CHUNKS):
        if c * CHUNK >= KEPT:
            copies[c - KEPT // CHUNK].wait()
        for i in range(c * CHUNK, (c + 1) * CHUNK):
            mask = (lane == i).astype(jnp.float32)[:1].astype(jnp.bfloat16)
            update = jnp.dot(both * mask, twice, preferred_element_type=jnp.float32)
            at = i // 2 * 8 + i % 2
            new[i] = keep[:, at : at + 1] * (*kept, *rest)[c][i - c * CHUNK] + update
        stores.append(
            pltpu.make_async_copy(
                new.at[pl.ds(c * CHUNK, CHUNK)], new_hbm.at[pl.ds(c * CHUNK, CHUNK)], out_sems.at[c]
            )
        )
        stores[-1].start()
    for store in stores:
        store.wait()


VMEM = pl.BlockSpec(memory_space=pltpu.VMEM)
ANY = pl.BlockSpec(memory_space=pl.ANY)


def hidden_of(q, k, ko, v, vo, ig, fg, igo, fgo, accepted, smax, norm, gain, *kept, state):
    return pl.pallas_call(
        hidden_kernel,
        in_specs=[VMEM] * (13 + len(kept)) + [ANY],
        out_specs=(VMEM, VMEM, VMEM),
        out_shape=(
            pltpu.VMEM((PROPS, SEQS, HEADS * DV), jnp.bfloat16),
            pltpu.VMEM((8, RUN), jnp.float32),
            pltpu.VMEM((RUN, DV), jnp.bfloat16),
        ),
        scratch_shapes=[
            *[pltpu.VMEM((CHUNK, DK, DV), jnp.float32)] * ((ITEMS - KEPT) // CHUNK),
            pltpu.VMEM((2, ROWS, DK), jnp.float32),
            pltpu.SemaphoreType.DMA((CHUNKS,)),
        ],
        name="hidden",
    )(q, k, ko, v, vo, ig, fg, igo, fgo, accepted, smax, norm, gain, *kept, state)


def memory_of(coef, k, ko, v, norm, *kept, state):
    return pl.pallas_call(
        memory_kernel,
        in_specs=[VMEM] * (5 + len(kept)) + [ANY],
        out_specs=(ANY, ANY, ANY),
        out_shape=(
            jax.ShapeDtypeStruct((ITEMS, DK, DV), jnp.float32),
            jax.ShapeDtypeStruct((ITEMS, DK), jnp.float32),
            jax.ShapeDtypeStruct((HEADS, SEQS), jnp.float32),
        ),
        scratch_shapes=[
            *[pltpu.VMEM((CHUNK, DK, DV), jnp.float32)] * ((ITEMS - KEPT) // CHUNK),
            pltpu.VMEM((ITEMS, DK, DV), jnp.float32),
            pltpu.VMEM((ITEMS, DK), jnp.float32),
            pltpu.VMEM((HEADS, SEQS), jnp.float32),
            pltpu.SemaphoreType.DMA((CHUNKS,)),
            pltpu.SemaphoreType.DMA((CHUNKS + 2,)),
        ],
        name="memory",
    )(coef, k, ko, v, norm, *kept, state)


def front_kernel(block_hbm, *refs):
    *refs, block, pieces, sems = refs
    count = (len(refs) - 2 - KEPT // CHUNK) // 2
    inputs, state_hbm, pieces_hbm, outputs = (
        refs[:count], refs[count], refs[count + 1], refs[count + 2 :]
    )
    first = pltpu.make_async_copy(block_hbm, block, sems.at[0])
    first.start()
    copies = [
        pltpu.make_async_copy(src, dst, sems.at[i + 2])
        for i, (src, dst) in enumerate(zip(inputs, outputs))
    ]
    copies += [
        pltpu.make_async_copy(
            state_hbm.at[pl.ds(i * CHUNK, CHUNK)], dst, sems.at[len(inputs) + i + 2]
        )
        for i, dst in enumerate(outputs[len(inputs) :])
    ]
    for copy in copies:
        copy.start()
    first.wait()
    for i in range(pieces.shape[0]):
        pieces[i] = block[...]
    last = pltpu.make_async_copy(pieces, pieces_hbm, sems.at[1])
    last.start()
    for copy in copies:
        copy.wait()
    last.wait()


def front(block, count, arrays, state):
    shape = (count, *block.shape)
    outs = [pltpu.VMEM(a.shape, a.dtype) for a in arrays]
    outs += [pltpu.VMEM((CHUNK, *state.shape[1:]), state.dtype)] * (KEPT // CHUNK)
    return pl.pallas_call(
        front_kernel,
        in_specs=[ANY] * (2 + len(arrays)),
        out_specs=[ANY] + [VMEM] * len(outs),
        out_shape=[jax.ShapeDtypeStruct(shape, block.dtype), *outs],
        scratch_shapes=[
            pltpu.VMEM(block.shape, block.dtype),
            pltpu.VMEM(shape, block.dtype),
            pltpu.SemaphoreType.DMA((2 + len(outs),)),
        ],
        name="front",
    )(block, *arrays, state)


def product_kernel(rows_ref, weight_ref, out_ref, *, order):
    terms = dot_bt(rows_ref[...], weight_ref[...]).astype(jnp.bfloat16)
    for i, source in enumerate(order):
        out_ref[i] = terms[source * SEQS : (source + 1) * SEQS]


def product(rows, weight, order):
    return pl.pallas_call(
        functools.partial(product_kernel, order=order),
        in_specs=[VMEM, VMEM],
        out_specs=VMEM,
        out_shape=pltpu.VMEM((len(order), SEQS, weight.shape[0]), jnp.bfloat16),
        name="product",
    )(rows, weight)


def join_kernel(terms_ref, out_ref, *, order, tps, block):
    cross = len(order) // tps
    slot = {source: i for i, source in enumerate(order)}
    lane = iota((SEQS, DK), 1) // block
    for part in range(terms_ref.shape[2] // DK):
        cols = slice(part * DK, (part + 1) * DK)
        sums = [
            sum(terms_ref[slot[g * tps + t], :, cols].astype(jnp.float32) for t in range(tps))
            for g in range(cross)
        ]
        step = 1
        while step < cross:
            low = lane & step == 0
            swapped = list(sums)
            for g in range(cross):
                if g & step == 0:
                    a, b = sums[g], sums[g + step]
                    swapped[g] = jnp.where(low, a, pltpu.roll(b, step * block, 1))
                    swapped[g + step] = jnp.where(low, pltpu.roll(a, DK - step * block, 1), b)
            sums = swapped
            step *= 2
        for z in range(cross):
            at = Z_ORDER[part * cross + z] * DK
            out_ref[:, at : at + DK] = sums[z].astype(jnp.bfloat16)


def joined(terms, order, tps, block):
    sources, seqs, cols = terms.shape
    return pl.pallas_call(
        functools.partial(join_kernel, order=order, tps=tps, block=block),
        in_specs=[VMEM],
        out_specs=VMEM,
        out_shape=jax.ShapeDtypeStruct((seqs, sources // tps * cols), jnp.bfloat16),
        name="join",
    )(terms)


def exchanged(pieces, axes, order):
    return lax.all_to_all(
        pieces, axes, split_axis=0, concat_axis=0, tiled=True, axis_index_groups=[order]
    )


def from_place(first, size):
    return [(first + i) % size for i in range(size)]


def in_vmem(array):
    return pltpu.with_memory_space_constraint(array, pltpu.VMEM)


def on_device(
    queries,
    keys,
    values,
    in_gate,
    forget_pre,
    old_keys,
    old_values,
    old_in_gate,
    old_forget,
    accepted,
    state_mem,
    state_norm,
    state_max,
    norm_gain,
    out_weight,
):
    zs, cross, tps = lax.axis_size("kv_0"), lax.axis_size(PLANE), lax.axis_size("tp")
    q, k, ko = (a.reshape(ROWS, DK) for a in (queries, keys, old_keys))
    v, vo = (
        a.reshape(SEQS, PROPS, HEADS, 2, DK).swapaxes(2, 3).reshape(RUN, DK)
        for a in (values, old_values)
    )
    gates = (
        a.transpose(1, 2, 0) for a in (in_gate, forget_pre, old_in_gate, old_forget)
    )
    norm = state_norm.reshape(ITEMS, DK)
    state = state_mem.reshape(ITEMS, DK, DV)
    inputs = (q, k, ko, v, vo, *gates, accepted[None], state_max.T, norm, norm_gain)
    pieces, *inputs = front(out_weight.T, zs, inputs, state)
    inputs = [in_vmem(a) for a in inputs]
    q, k, ko = inputs[:3]
    norm, kept = inputs[11], inputs[13:]
    weight = exchanged(pieces, "kv_0", list(Z_ORDER))
    weight = weight.reshape(-1, out_weight.shape[0])
    hidden, coef, run_values = hidden_of(*inputs, state=state)
    rows = lax.all_gather(hidden.reshape(PROPS * SEQS, -1), PLANE, tiled=True)
    order = [g * tps + t for g in from_place(FIRST_CROSS, cross) for t in from_place(FIRST_TP, tps)]
    terms = product(in_vmem(rows), in_vmem(weight), order)
    terms = exchanged(terms, (*PLANE, "tp"), order)
    new_mem, new_norm, new_max = memory_of(
        in_vmem(coef), k, ko, in_vmem(run_values), norm, *kept, state=state
    )
    mixed = joined(in_vmem(terms), order, tps, out_weight.shape[1])[:, None]
    return (
        mixed,
        new_mem.reshape(state_mem.shape),
        new_norm.reshape(state_norm.shape),
        new_max.T,
    )


def solution(mesh):
    finer = Mesh(mesh.devices.reshape(16, 4, 2, mesh.shape["tp"]), (*KV, "tp"))
    in_specs = (
        P(KV, None, "tp", None),
        P(KV, None, "tp", None),
        P(KV, None, "tp", None),
        P(KV, None, "tp"),
        P(KV, None, "tp"),
        P(KV, None, "tp", None),
        P(KV, None, "tp", None),
        P(KV, None, "tp"),
        P(KV, None, "tp"),
        P(KV),
        P(KV, "tp", None, None),
        P(KV, "tp", None),
        P(KV, "tp"),
        P("tp", None),
        P("tp", KV),
    )
    out_specs = (P(KV, "tp", None), P(KV, "tp", None, None), P(KV, "tp", None), P(KV, "tp"))
    return jax.shard_map(
        on_device, mesh=finer, in_specs=in_specs, out_specs=out_specs, check_vma=False
    )
```
